512 devices in a mesh: ep: 16 (over y, x), tp: 32 (over z, core).
Axes of the slice: x: 4, y: 4, z: 16, core: 2. Of those that a mesh axis runs over, the one named last changes fastest.
Arguments:
- tokens: bfloat16 [3072, 2048], P('ep'), may hold values from -6 to 6
- cotangent: bfloat16 [3072, 2048], P('ep'), may hold values from -6 to 6
- routes: int32 [3072, 2], P('ep'), may hold values from 0 to 15, all different within a row; in each aligned block of 192 rows (0 to 191, 192 to 383, ...) at most 48 rows name the same one
- route_weight: float32 [3072, 2], P('ep'), may hold values from 0.2 to 1
- gate_weight: bfloat16 [16, 2048, 4096], P('ep', None, 'tp'), may hold values from -0.125 to 0.125
- up_weight: bfloat16 [16, 2048, 4096], P('ep', None, 'tp'), may hold values from -0.125 to 0.125
- down_weight: bfloat16 [16, 4096, 2048], P('ep', 'tp'), may hold values from -0.09375 to 0.09375
Outputs:
- grad_tokens: bfloat16 [3072, 2048], P('ep', 'tp')
- grad_route: float32 [3072, 2], P('ep')
- grad_gate: bfloat16 [16, 2048, 4096], P('ep', None, 'tp')
- grad_up: bfloat16 [16, 2048, 4096], P('ep', None, 'tp')
- grad_down: bfloat16 [16, 4096, 2048], P('ep', 'tp')
The draws below stay inside these ranges and needn't reach their ends.
Inputs may be any that keep to these rules, and one draw needn't show every extreme that they name: `routes`: within the rows of one device along ep, each expert is named at most 48 times, a bound that some block reaches; the 2 entries of a row differ.
All inputs are finite; a program needn't handle non-finite values.
Results may differ from the reference program's by a relative error of at most 0.025.
Values may be sent and summed in bfloat16 or wider, within the bound.
No kernel may reach another device: no remote copies, remote signals or barrier semaphores. Data moves between devices by JAX's collectives and lax.ppermute only.
A program may use at most 64 MiB of HBM per device.

```python
import math
import jax
import jax.numpy as jnp
import numpy as np
from jax import lax

D = 2048
FF = 4096
TOP = 2
TOK_DEV = 192
EXPERTS = 16
TOKENS = 3072
CAP = 48
N_EP = 16
N_TP = 32


def shard_levels(key, extent, shards, least, largest):
    loudness, own = 1.0, jax.random.fold_in(key, 6)
    for axis_at, blocks in shards:
        steps = jnp.exp(jax.random.uniform(jax.random.fold_in(own, axis_at), (blocks,), jnp.float32, least / len(shards), largest / len(shards)))
        loudness = loudness * jnp.repeat(steps, extent[axis_at] // blocks).reshape([-1 if axis == axis_at else 1 for axis in range(len(extent))])
    return loudness


def assign_block(rng, own, number, rows, count, top, reach, lean):
    ranking = jax.random.permutation(rng, count)
    crowded, usual = shares(count, rows * top, reach, lean, True), shares(count, rows * top, reach, lean, False)
    places = jnp.arange(count)

    def named(sizes, turn):
        used = int((sizes > 0).sum())
        fixed = max(1, used // 4)
        passed = fixed + (places - fixed + turn * (used - fixed)) % max(1, count - fixed)
        return jnp.zeros((count,), jnp.int32).at[ranking[jnp.where(places < fixed, places, passed)]].set(jnp.asarray(sizes, jnp.int32))

    sizes = jnp.where(number % 4 == 0, named(crowded, number // 4), named(usual, number - number // 4 - 1))
    mixed = jax.random.permutation(jax.random.fold_in(own, 3), count)
    source_of, taker = mixed[0:count // 2 * 2:2], mixed[1:count // 2 * 2:2]
    slack = jnp.minimum(sizes[source_of] - 1, reach - sizes[taker]) // 2
    slack = jnp.where((source_of == ranking[0]) | (taker == ranking[0]) | (sizes[taker] == 0), 0, jnp.maximum(slack, 0))
    passed = jax.random.randint(jax.random.fold_in(own, 4), (count // 2,), 0, 1 << 20) % (slack + 1)
    sizes = sizes.at[source_of].add(-passed).at[taker].add(passed)
    items = jnp.searchsorted(jnp.cumsum(sizes), jnp.arange(rows * top), side="right").astype(jnp.int32)
    listing = items.reshape(top, rows).T
    listing = listing[jax.random.permutation(jax.random.fold_in(own, 1), rows)]
    turn = jax.random.randint(jax.random.fold_in(own, 2), (rows, 1), 0, top)
    return jnp.take_along_axis(listing, (jnp.arange(top)[None, :] + turn) % top, axis=1)


def shares(count, total, reach, slope, full):
    weights = [(1 << 20) // math.isqrt(grade ** slope) + 1 for grade in range(1, count + 1)]
    largest = reach if full else min(reach, max(-(-total // count), total * weights[0] // sum(weights)))
    least = 1 if total - largest >= count - 1 else 0
    holding, rest = [largest] + [least] * (count - 1), total - largest - least * (count - 1)
    while rest > 0:
        candidates = [i for i in range(1, count) if holding[i] < largest] or [i for i in range(1, count) if holding[i] < reach]
        whole, remaining = sum([weights[i] for i in candidates]), rest
        for i in candidates:
            addition = min(reach - holding[i], max(1, remaining * weights[i] // whole), rest)
            holding[i] = holding[i] + addition
            rest = rest - addition
    return np.array(holding)


def gaussian(own_key, shape, deviation, most, cuts=(), kind=jnp.bfloat16):
    array = jax.random.normal(own_key, shape, jnp.float32) * deviation
    if len(cuts) > 0:
        array = shard_levels(own_key, shape, cuts, -0.22, 0.18) * array
    return jnp.clip(array, min=-most, max=most).astype(kind)


def setup_inputs(seed: int = 0) -> dict:
    seeds = jax.random.split(jax.random.key(seed), 8)
    tokens = gaussian(seeds[0], (TOKENS, D), 1.0, 6.0, ((0, 16),))
    cotangent = gaussian(seeds[1], (TOKENS, D), 1.0, 6.0, ((0, 16),))
    routes_keys = jax.random.split(jax.random.fold_in(seeds[2], 1), TOKENS // TOK_DEV)
    routes_turns = jax.random.permutation(jax.random.fold_in(seeds[2], 3), TOKENS // TOK_DEV)
    routes = jax.vmap(lambda own, number: assign_block(jax.random.fold_in(seeds[2], 2), own, number, TOK_DEV, EXPERTS, TOP, CAP, 2))(routes_keys, routes_turns).reshape((TOKENS, TOP))
    route_weight = jnp.clip(0.2 + 0.8 * jax.random.uniform(seeds[3], (TOKENS, TOP), jnp.float32) ** shard_levels(seeds[3], (TOKENS, TOP), ((0, 16),), -0.2, 0.2), 0.2, 1.0)
    gate_weight = gaussian(seeds[4], (EXPERTS, D, FF), D ** -0.5, 0.125, ((0, 16), (2, 32)))
    up_weight = gaussian(seeds[5], (EXPERTS, D, FF), D ** -0.5, 0.125, ((0, 16), (2, 32)))
    down_weight = gaussian(seeds[6], (EXPERTS, FF, D), FF ** -0.5, 0.09375, ((0, 16), (1, 32)))
    return dict(tokens=tokens, cotangent=cotangent, routes=routes, route_weight=route_weight, gate_weight=gate_weight, up_weight=up_weight, down_weight=down_weight)


def slot_layout(routes):
    flat_routes = routes.reshape(N_EP, TOK_DEV * TOP).astype(jnp.int32)
    expert_ids = jnp.arange(EXPERTS, dtype=jnp.int32)
    onehot_table = (flat_routes[:, :, None] == expert_ids[None, None, :]).astype(jnp.int32)
    earlier = jnp.cumsum(onehot_table, axis=1) - onehot_table
    order_in = jnp.sum(earlier * onehot_table, axis=2).astype(jnp.int32)
    source_block = jnp.arange(N_EP, dtype=jnp.int32)[:, None]
    position = (source_block * CAP + order_in).astype(jnp.int32)
    entries = jnp.arange(N_EP * TOK_DEV * TOP, dtype=jnp.int32).reshape(N_EP, TOK_DEV * TOP) + 1
    slot_table = jnp.zeros((EXPERTS, N_EP * CAP), jnp.int32).at[flat_routes, position].set(entries)
    return slot_table


def expert_step(x_rows, c_rows, w_rows, w_gate, w_upper, w_lower):
    gate_pre = jnp.dot(x_rows, w_gate, preferred_element_type=jnp.float32)
    up_pre = jnp.dot(x_rows, w_upper, preferred_element_type=jnp.float32)
    sig = jax.nn.sigmoid(gate_pre)
    active = gate_pre * sig
    hidden = (active * up_pre).astype(jnp.bfloat16)
    back_raw = jnp.dot(c_rows, w_lower.T, preferred_element_type=jnp.float32)
    route_part = jnp.sum(hidden.astype(jnp.float32) * back_raw, axis=1)
    scaled_back = w_rows[:, None] * back_raw
    grad_gate_pre = (scaled_back * up_pre * sig * (1.0 + gate_pre * (1.0 - sig))).astype(jnp.bfloat16)
    grad_up_pre = (scaled_back * active).astype(jnp.bfloat16)
    scaled_cot = (w_rows[:, None] * c_rows.astype(jnp.float32)).astype(jnp.bfloat16)
    grad_wg = jnp.dot(x_rows.T, grad_gate_pre, preferred_element_type=jnp.float32).astype(jnp.bfloat16)
    grad_wu = jnp.dot(x_rows.T, grad_up_pre, preferred_element_type=jnp.float32).astype(jnp.bfloat16)
    grad_wd = jnp.dot(hidden.T, scaled_cot, preferred_element_type=jnp.float32).astype(jnp.bfloat16)
    group_width = FF // N_TP

    def add_group(group, total):
        lower = (group * group_width).astype(jnp.int32)
        part = jnp.dot(lax.dynamic_slice_in_dim(grad_gate_pre, lower, group_width, 1),
                       lax.dynamic_slice_in_dim(w_gate, lower, group_width, 1).T,
                       preferred_element_type=jnp.float32)
        part = part + jnp.dot(lax.dynamic_slice_in_dim(grad_up_pre, lower, group_width, 1),
                              lax.dynamic_slice_in_dim(w_upper, lower, group_width, 1).T,
                              preferred_element_type=jnp.float32)
        return total + lax.optimization_barrier(part.astype(jnp.bfloat16)).astype(jnp.float32)

    start_total = jnp.zeros((x_rows.shape[0], D), jnp.float32)
    row_total = lax.fori_loop(jnp.int32(0), jnp.int32(N_TP), add_group, start_total)
    return grad_wg, grad_wu, grad_wd, row_total.astype(jnp.bfloat16), route_part


def reference(tokens, cotangent, routes, route_weight, gate_weight, up_weight, down_weight):
    slot_table = slot_layout(routes)
    filled = slot_table > 0
    entry = jnp.maximum(slot_table - 1, 0).astype(jnp.int32)
    flat_weight = route_weight.reshape(-1)

    def per_expert(args):
        filled_e, entry_e, w_gate, w_upper, w_lower = args
        source_row = (entry_e // TOP).astype(jnp.int32)
        x_rows = jnp.where(filled_e[:, None], tokens[source_row], jnp.zeros((), jnp.bfloat16)).astype(jnp.bfloat16)
        c_rows = jnp.where(filled_e[:, None], cotangent[source_row], jnp.zeros((), jnp.bfloat16)).astype(jnp.bfloat16)
        w_round = jnp.where(filled_e, flat_weight[entry_e], jnp.zeros((), jnp.float32)).astype(jnp.bfloat16)
        w_rows = lax.optimization_barrier(w_round).astype(jnp.float32)
        return expert_step(x_rows, c_rows, w_rows, w_gate, w_upper, w_lower)

    grad_gate, grad_up, grad_down, row_grads, route_parts = lax.map(
        per_expert, (filled, entry, gate_weight, up_weight, down_weight))
    target = jnp.where(filled, slot_table - 1, TOKENS * TOP).astype(jnp.int32).reshape(-1)
    flat_rows = jnp.zeros((TOKENS * TOP, D), jnp.bfloat16).at[target].set(row_grads.reshape(-1, D), mode="drop")
    grad_tokens = jnp.sum(flat_rows.reshape(TOKENS, TOP, D).astype(jnp.float32), axis=1).astype(jnp.bfloat16)
    flat_route = jnp.zeros((TOKENS * TOP,), jnp.float32).at[target].set(route_parts.reshape(-1), mode="drop")
    grad_route = flat_route.reshape(TOKENS, TOP)
    return grad_tokens, grad_route, grad_gate, grad_up, grad_down
```

```python
import functools

import jax
import jax.numpy as jnp
from jax import lax
from jax.experimental import pallas as pl
from jax.experimental.pallas import tpu as pltpu
from jax.sharding import Mesh
from jax.sharding import PartitionSpec as P

BF = jnp.bfloat16
F32 = jnp.float32
TP = ("zh", "zl", "core")
LANES = 128
OWN = 64


def dot(a, b, ca=1, cb=0):
    return lax.dot_general(a, b, (((ca,), (cb,)), ((), ())), preferred_element_type=F32)


def split(v):
    hi = v.astype(BF)
    return hi, (v - hi.astype(F32)).astype(BF)


def padded(v, width):
    return jnp.concatenate([v, jnp.zeros((v.shape[0], width - v.shape[1]), v.dtype)], axis=1)


def stacked(rows, height):
    place = lax.broadcasted_iota(jnp.int32, (height, rows[0].shape[1]), 0)
    out = jnp.zeros(place.shape, F32)
    for k, row in enumerate(rows):
        out = jnp.where(place == k, row.astype(F32), out)
    return out


def ranks(routes, experts):
    rows = routes.shape[1]
    ids = lax.broadcasted_iota(jnp.int32, (experts, rows), 0)
    first, second = routes[0:1] == ids, routes[1:2] == ids
    named = first | second
    before = lax.broadcasted_iota(jnp.int32, (rows, rows), 0) < lax.broadcasted_iota(
        jnp.int32, (rows, rows), 1
    )
    one, zero = jnp.ones((), F32), jnp.zeros((), F32)
    count = dot(jnp.where(named, one, zero).astype(BF), jnp.where(before, one, zero).astype(BF))
    return first, second, jnp.where(named, count, -one)


def pack_kernel(core, routes, weights, x, c, out, sel, wsel, *, experts, cap, chunks):
    i = pl.program_id(0)

    @pl.when(i == 0)
    def _():
        first, second, rank = ranks(routes[...], experts)
        w = weights[...]
        mine = jnp.where(first, w[0:1], 0.0) + jnp.where(second, w[1:2], 0.0)
        slot = lax.broadcasted_iota(jnp.int32, (cap, rank.shape[1]), 0).astype(F32)
        for e in range(experts):
            hit = rank[e : e + 1] == slot
            sel[pl.ds(e * cap, cap), :] = jnp.where(hit, 1.0, 0.0).astype(BF)
            wsel[pl.ds(e * cap, cap), :] = jnp.where(hit, mine[e : e + 1], 0.0).astype(BF)

    @pl.when(i < chunks)
    def _():
        out[...] = dot(sel[...], x[...]).astype(BF)

    @pl.when(i >= chunks)
    def _():
        out[...] = dot(wsel[...], c[...]).astype(BF)


def pack(core, routes, weights, tokens, cot, experts, cap, width):
    rows, d = tokens.shape
    chunks = d // 2 // width
    slots = experts * cap
    whole = lambda i, c: (0, 0)
    return pl.pallas_call(
        functools.partial(pack_kernel, experts=experts, cap=cap, chunks=chunks),
        grid_spec=pltpu.PrefetchScalarGridSpec(
            num_scalar_prefetch=1,
            grid=(2 * chunks,),
            in_specs=[
                pl.BlockSpec((2, rows), whole),
                pl.BlockSpec((2, rows), whole),
                pl.BlockSpec((rows, width), lambda i, c: (0, c[0] * chunks + jnp.minimum(i, chunks - 1))),
                pl.BlockSpec((rows, width), lambda i, c: (0, c[0] * chunks + jnp.maximum(i - chunks, 0))),
            ],
            out_specs=[
                pl.BlockSpec((slots, width), lambda i, c: (0, i)),
                pl.BlockSpec((slots, rows), whole),
            ],
            scratch_shapes=[pltpu.VMEM((slots, rows), BF)],
        ),
        out_shape=[
            jax.ShapeDtypeStruct((slots, d), BF),
            jax.ShapeDtypeStruct((slots, rows), BF),
        ],
        name="pack",
    )(core, routes, weights, tokens, cot)


def ordered(five, out, col):
    nzh, nzl = five.shape[0], five.shape[1]
    for zl in range(nzl):
        for zh in range(nzh):
            out[pl.ds((zl * nzh + zh) * OWN, OWN), pl.ds(col, LANES)] = five[zh, zl, 0]


def main_kernel(core, ox, oc, tx, tc, g0, g1, u0, u1, d0, d1, g5, u5,
                hid, dd, dx, rt, wgu, wp):
    half = g0.shape[0]

    @pl.when(pl.program_id(0) == 0)
    def _():
        wgu[pl.ds(0, half), pl.ds(0, LANES)] = g0[...]
        wgu[pl.ds(half, half), pl.ds(0, LANES)] = g1[...]
        wgu[pl.ds(0, half), pl.ds(LANES, LANES)] = u0[...]
        wgu[pl.ds(half, half), pl.ds(LANES, LANES)] = u1[...]
        ordered(g5, wp, 0)
        ordered(u5, wp, LANES)

    ab = dot(ox[...], wgu[pl.ds(0, half), :]) + dot(tx[...], wgu[pl.ds(half, half), :])
    back = dot(oc[...], d0[...], 1, 1) + dot(tc[...], d1[...], 1, 1)
    a, b = ab[:, :LANES], ab[:, LANES:]
    s = jax.nn.sigmoid(a)
    act = a * s
    hidden = (act * b).astype(BF)
    da = (back * b * s * (1.0 + a * (1.0 - s))).astype(BF)
    db = (back * act).astype(BF)
    both = jnp.concatenate([da, db], axis=1)
    hid[...] = hidden
    dd[...] = both
    n = hidden.shape[0]
    route = jnp.sum((hidden.astype(F32) * back).T, axis=0, keepdims=True)
    route = padded(route, rt.shape[1])
    rt[...] = stacked([route], 8)
    dx[pl.ds(0, n), :] = dot(both, wp[...], 1, 1).astype(BF)
    tail = stacked(split(route), 8).astype(BF)
    dx[pl.ds(n, 8), pl.ds(0, rt.shape[1])] = tail
    if dx.shape[1] > rt.shape[1]:
        rest = dx.shape[1] - rt.shape[1]
        dx[pl.ds(n, 8), pl.ds(rt.shape[1], rest)] = jnp.zeros((8, rest), BF)


def main(core, own, oth, gate, up, down, nzh, nzl, block):
    slots, d = own.shape
    half = d // 2
    steps = slots // block
    lanes = -(-block // LANES) * LANES
    g5 = gate.reshape(nzh, nzl, 2, OWN, LANES)
    u5 = up.reshape(nzh, nzl, 2, OWN, LANES)
    five = pl.BlockSpec((nzh, nzl, 1, OWN, LANES), lambda i, c: (0, 0, 1 - c[0], 0, 0))
    rows0 = pl.BlockSpec((half, LANES), lambda i, c: (c[0], 0))
    rows1 = pl.BlockSpec((half, LANES), lambda i, c: (1 - c[0], 0))
    left = pl.BlockSpec((block, half), lambda i, c: (i, 0))
    right = pl.BlockSpec((block, half), lambda i, c: (i, 1))
    at = lambda i, c: (i, 0)
    return pl.pallas_call(
        main_kernel,
        grid_spec=pltpu.PrefetchScalarGridSpec(
            num_scalar_prefetch=1,
            grid=(steps,),
            in_specs=[
                left, right, left, right, rows0, rows1, rows0, rows1,
                pl.BlockSpec((LANES, half), lambda i, c: (0, c[0])),
                pl.BlockSpec((LANES, half), lambda i, c: (0, 1 - c[0])),
                five, five,
            ],
            out_specs=[
                pl.BlockSpec((block, LANES), at),
                pl.BlockSpec((block, 2 * LANES), at),
                pl.BlockSpec((block + 8, half), at),
                pl.BlockSpec((8, lanes), at),
            ],
            scratch_shapes=[pltpu.VMEM((d, 2 * LANES), BF), pltpu.VMEM((half, 2 * LANES), BF)],
        ),
        out_shape=[
            jax.ShapeDtypeStruct((slots, LANES), BF),
            jax.ShapeDtypeStruct((slots, 2 * LANES), BF),
            jax.ShapeDtypeStruct((steps * (block + 8), half), BF),
            jax.ShapeDtypeStruct((steps * 8, lanes), F32),
        ],
        name="expert",
    )(core, own, own, oth, oth, gate, gate, up, up, down, down, g5, u5)


def grads_kernel(core, ox, oc, tx, tc, hid, dd, gg, gu, gd, *, chunks):
    def step(x, c):
        both = dot(x[...], dd[...], 0, 0)
        gg[...] = both[:, :LANES].astype(BF)
        gu[...] = both[:, LANES:].astype(BF)
        gd[...] = dot(hid[...], c[...], 0, 0).astype(BF)

    i = pl.program_id(0)

    @pl.when(i < chunks)
    def _():
        step(ox, oc)

    @pl.when(i >= chunks)
    def _():
        step(tx, tc)


def grads(core, own, oth, hid, dd, width):
    slots, d = own.shape
    chunks = d // 2 // width
    first = lambda i: jnp.minimum(i, chunks - 1)
    last = lambda i: jnp.maximum(i - chunks, 0)
    place = lambda i, c: jnp.where(i < chunks, c[0] * chunks + i, (1 - c[0]) * chunks + i - chunks)
    col = lambda f: pl.BlockSpec((slots, width), f)
    whole = lambda i, c: (0, 0)
    return pl.pallas_call(
        functools.partial(grads_kernel, chunks=chunks),
        grid_spec=pltpu.PrefetchScalarGridSpec(
            num_scalar_prefetch=1,
            grid=(2 * chunks,),
            in_specs=[
                col(lambda i, c: (0, first(i))),
                col(lambda i, c: (0, chunks + first(i))),
                col(lambda i, c: (0, last(i))),
                col(lambda i, c: (0, chunks + last(i))),
                pl.BlockSpec((slots, LANES), whole),
                pl.BlockSpec((slots, 2 * LANES), whole),
            ],
            out_specs=[
                pl.BlockSpec((width, LANES), lambda i, c: (place(i, c), 0)),
                pl.BlockSpec((width, LANES), lambda i, c: (place(i, c), 0)),
                pl.BlockSpec((LANES, width), lambda i, c: (0, place(i, c))),
            ],
        ),
        out_shape=[
            jax.ShapeDtypeStruct((d, LANES), BF),
            jax.ShapeDtypeStruct((d, LANES), BF),
            jax.ShapeDtypeStruct((LANES, d), BF),
        ],
        cost_estimate=pl.CostEstimate(
            flops=2 * slots * d * 3 * LANES, bytes_accessed=slots * d * 4, transcendentals=0
        ),
        name="weight_grads",
    )(core, own, own, oth, oth, hid, dd)


def send_kernel(core, got, dd, rt, g5, u5, out, wp, *, cap):
    @pl.when(pl.program_id(0) == 0)
    def _():
        ordered(g5, wp, 0)
        ordered(u5, wp, LANES)

    n = dd.shape[0]
    lanes = rt.shape[1]
    nzl = g5.shape[1]
    per = wp.shape[0] // nzl // LANES
    total = (dot(dd[...], wp[...], 1, 1) + got[pl.ds(0, n), :].astype(F32)).astype(BF)
    tail = got[pl.ds(n, 8), pl.ds(0, lanes)].astype(F32)
    route = rt[0:1] + tail[0:1] + tail[1:2]
    for b in range(n // cap):
        ends = stacked(split(padded(route[:, b * cap : (b + 1) * cap], LANES)), 8).astype(BF)
        for zl in range(nzl):
            for q in range(per):
                k = zl * per + q
                out[b * nzl + zl, pl.ds(q * cap, cap), :] = total[
                    b * cap : (b + 1) * cap, k * LANES : (k + 1) * LANES
                ]
            out[b * nzl + zl, pl.ds(per * cap, 8), :] = ends


def send(core, got, dd, rt, gate, up, nzh, nzl, cap, block):
    slots = dd.shape[0]
    half = got.shape[1]
    steps = slots // block
    lanes = rt.shape[1]
    g5 = gate.reshape(nzh, nzl, 2, OWN, LANES)
    u5 = up.reshape(nzh, nzl, 2, OWN, LANES)
    five = pl.BlockSpec((nzh, nzl, 1, OWN, LANES), lambda i, c: (0, 0, c[0], 0, 0))
    tall = half // nzl // LANES * cap + 8
    at = lambda i, c: (i, 0)
    return pl.pallas_call(
        functools.partial(send_kernel, cap=cap),
        grid_spec=pltpu.PrefetchScalarGridSpec(
            num_scalar_prefetch=1,
            grid=(steps,),
            in_specs=[
                pl.BlockSpec((block + 8, half), at),
                pl.BlockSpec((block, 2 * LANES), at),
                pl.BlockSpec((8, lanes), at),
                five, five,
            ],
            out_specs=pl.BlockSpec((block // cap * nzl, tall, LANES), lambda i, c: (i, 0, 0)),
            scratch_shapes=[pltpu.VMEM((half, 2 * LANES), BF)],
        ),
        out_shape=jax.ShapeDtypeStruct((slots // cap * nzl, tall, LANES), BF),
        name="send",
    )(core, got, dd, rt, g5, u5)


def combine_kernel(routes, weights, sel, got, out, part, *, experts, cap, nzl):
    rows = routes.shape[1]
    per = (got.shape[1] - 8) // cap
    s = sel[...]
    total = None
    for zl in range(nzl):
        for e in range(experts):
            for q in range(per):
                part[zl, pl.ds(e * cap, cap), pl.ds(q * LANES, LANES)] = got[
                    e * nzl + zl, pl.ds(q * cap, cap), :
                ]
        one = dot(s, part[zl], 0, 0)
        total = one if total is None else total + one
    total = total.astype(BF)
    mid = rows // 2
    for k in range(out.shape[0]):
        out[k, pl.ds(0, mid), :] = jnp.concatenate(
            [total[:mid, k * OWN : (k + 1) * OWN], total[mid:, k * OWN : (k + 1) * OWN]], axis=1
        )
    lines = []
    for e in range(experts):
        line = jnp.zeros((1, LANES), F32)
        for zl in range(nzl):
            tail = got[e * nzl + zl, pl.ds(per * cap, 8), :].astype(F32)
            line = line + tail[0:1] + tail[1:2]
        lines.append(line)
    r_hi, r_lo = split(stacked(lines, max(experts, 8)))
    first, second, rank = ranks(routes[...], experts)
    slot = lax.broadcasted_iota(jnp.int32, (LANES, rows), 0).astype(F32)
    ends = []
    wide = -(-rows // LANES) * LANES
    for ch, hit in enumerate((first, second)):
        place = jnp.sum(jnp.where(hit, rank, 0.0), axis=0, keepdims=True)
        pick = jnp.where(slot == place, 1.0, 0.0).astype(BF)
        value = (dot(r_hi, pick) + dot(r_lo, pick))[:experts]
        value = jnp.sum(jnp.where(hit, value, 0.0), axis=0, keepdims=True)
        w = weights[...][ch : ch + 1].astype(BF).astype(F32)
        for piece in split(padded(value / w, wide) if wide > rows else value / w):
            for k in range(wide // LANES):
                ends.append(piece[:, k * LANES : (k + 1) * LANES])
    ends = stacked(ends, 8).astype(BF)
    for k in range(out.shape[0]):
        out[k, pl.ds(mid, 8), :] = ends


def combine(routes, weights, sel, got, experts, cap, nzh, nzl):
    rows = routes.shape[1]
    per = (got.shape[1] - 8) // cap
    return pl.pallas_call(
        functools.partial(combine_kernel, experts=experts, cap=cap, nzl=nzl),
        out_shape=jax.ShapeDtypeStruct((nzh, rows // 2 + 8, LANES), BF),
        scratch_shapes=[pltpu.VMEM((nzl, experts * cap, per * LANES), BF)],
        name="combine",
    )(routes, weights, sel, got)


def finish_kernel(got, grad, route):
    rows = grad.shape[1]
    total = got[0].astype(F32)
    for k in range(1, got.shape[0]):
        total = total + got[k].astype(F32)
    mid = rows // 2
    turned = total[:mid].T
    grad[...] = jnp.concatenate([turned[:OWN], turned[OWN:]], axis=1).astype(BF)
    ends = total[mid:]
    n = -(-rows // LANES)
    for ch in range(2):
        pieces = [
            ends[2 * n * ch + k : 2 * n * ch + k + 1] + ends[2 * n * ch + n + k : 2 * n * ch + n + k + 1]
            for k in range(n)
        ]
        line = jnp.concatenate(pieces, axis=1) if n > 1 else pieces[0]
        route[pl.ds(ch, 1), :] = line[:, :rows]


def finish(got, rows):
    return pl.pallas_call(
        finish_kernel,
        out_shape=[
            jax.ShapeDtypeStruct((OWN, rows), BF),
            jax.ShapeDtypeStruct((2, rows), F32),
        ],
        name="finish",
    )(got)


def shards(tokens, cotangent, routes, route_weight, gate_weight, up_weight, down_weight):
    rows, d = tokens.shape
    experts = lax.axis_size("ep")
    nzh, nzl = lax.axis_size("zh"), lax.axis_size("zl")
    cap = 2 * rows * routes.shape[1] // experts
    slots = experts * cap
    block = min(4, experts, d // 2 // cap) * cap
    width = min(256, d // 2)
    core = lax.axis_index("core").astype(jnp.int32).reshape(1)
    routes_t, weight_t = routes.T, route_weight.T
    gate, up, down = gate_weight[0], up_weight[0], down_weight[0]
    swap = [(0, 1), (1, 0)]

    packed, sel = pack(core, routes_t, weight_t, tokens, cotangent, experts, cap, width)
    own = lax.all_to_all(packed.reshape(experts, cap, d), "ep", 0, 0, tiled=True).reshape(slots, d)
    oth = lax.ppermute(own, "core", swap)
    hid, dd, dx, rt = main(core, own, oth, gate, up, down, nzh, nzl, block)
    got = lax.ppermute(dx, "core", swap)
    gg, gu, gd = grads(core, own, oth, hid, dd, width)
    message = send(core, got, dd, rt, gate, up, nzh, nzl, cap, block)
    back = lax.all_to_all(message, ("ep", "zl"), 0, 0, tiled=True)
    partial = combine(routes_t, weight_t, sel, back, experts, cap, nzh, nzl)
    last = lax.all_to_all(partial, "zh", 0, 0, tiled=True)
    grad_t, route_t = finish(last, rows)
    return grad_t.T, route_t.T, gg[None], gu[None], gd[None]


def solution(mesh):
    devices = mesh.devices
    ep = devices.shape[0]
    finer = Mesh(devices.reshape(ep, -1, 2, 2), ("ep", "zh", "zl", "core"))
    in_specs = (
        P("ep", None),
        P("ep", None),
        P("ep", None),
        P("ep", None),
        P("ep", None, TP),
        P("ep", None, TP),
        P("ep", TP, None),
    )
    out_specs = (
        P("ep", TP),
        P("ep", None),
        P("ep", None, TP),
        P("ep", None, TP),
        P("ep", TP, None),
    )
    return jax.shard_map(
        shards, mesh=finer, in_specs=in_specs, out_specs=out_specs, check_vma=False
    )
```

```python
import functools

import jax
import jax.numpy as jnp
from jax import lax
from jax.experimental import pallas as pl
from jax.experimental.pallas import tpu as pltpu
from jax.sharding import Mesh
from jax.sharding import PartitionSpec as P

BF = jnp.bfloat16
F32 = jnp.float32
TP = ("zh", "zl", "core")
LANES = 128
OWN = 64


def dot(a, b, ca=1, cb=0):
    return lax.dot_general(a, b, (((ca,), (cb,)), ((), ())), preferred_element_type=F32)


def split(v):
    hi = v.astype(BF)
    return hi, (v - hi.astype(F32)).astype(BF)


def padded(v, width):
    return jnp.concatenate([v, jnp.zeros((v.shape[0], width - v.shape[1]), v.dtype)], axis=1)


def stacked(rows, height):
    place = lax.broadcasted_iota(jnp.int32, (height, rows[0].shape[1]), 0)
    out = jnp.zeros(place.shape, F32)
    for k, row in enumerate(rows):
        out = jnp.where(place == k, row.astype(F32), out)
    return out


def ranks(routes, experts):
    rows = routes.shape[1]
    ids = lax.broadcasted_iota(jnp.int32, (experts, rows), 0)
    first, second = routes[0:1] == ids, routes[1:2] == ids
    named = first | second
    before = lax.broadcasted_iota(jnp.int32, (rows, rows), 0) < lax.broadcasted_iota(
        jnp.int32, (rows, rows), 1
    )
    one, zero = jnp.ones((), F32), jnp.zeros((), F32)
    count = dot(jnp.where(named, one, zero).astype(BF), jnp.where(before, one, zero).astype(BF))
    return first, second, jnp.where(named, count, -one)


def vmem(n):
    return [pl.BlockSpec(memory_space=pltpu.VMEM)] * n


def call(kernel, name, out, scratch, limit, flops, *args):
    return pl.pallas_call(
        kernel,
        in_specs=[pl.BlockSpec(memory_space=pltpu.SMEM)] + vmem(len(args) - 1),
        out_specs=vmem(len(out)),
        out_shape=out,
        scratch_shapes=scratch,
        compiler_params=pltpu.CompilerParams(vmem_limit_bytes=limit << 20),
        cost_estimate=pl.CostEstimate(flops=flops, bytes_accessed=flops // 400, transcendentals=0),
        name=name,
    )(*args)


def struct(*shape, dtype=BF):
    return jax.ShapeDtypeStruct(shape, dtype)


def pack_kernel(core, routes, weights, x, c, out, sel, wsel, *, experts, cap):
    half = x.shape[1] // 2
    own = pl.ds(pl.multiple_of(core[0] * half, half), half)
    first, second, rank = ranks(routes[...], experts)
    w = weights[...]
    mine = jnp.where(first, w[0:1], 0.0) + jnp.where(second, w[1:2], 0.0)
    slot = lax.broadcasted_iota(jnp.int32, (cap, rank.shape[1]), 0).astype(F32)
    for e in range(experts):
        hit = rank[e : e + 1] == slot
        sel[pl.ds(e * cap, cap), :] = jnp.where(hit, 1.0, 0.0).astype(BF)
        wsel[pl.ds(e * cap, cap), :] = jnp.where(hit, mine[e : e + 1], 0.0).astype(BF)
    out[:, pl.ds(0, half)] = dot(sel[...], x[:, own]).astype(BF)
    out[:, pl.ds(half, half)] = dot(wsel[...], c[:, own]).astype(BF)


def pack(core, routes, weights, tokens, cot, experts, cap):
    rows, d = tokens.shape
    slots = experts * cap
    return call(
        functools.partial(pack_kernel, experts=experts, cap=cap),
        "pack", [struct(slots, d), struct(slots, rows)], [pltpu.VMEM((slots, rows), BF)],
        20, 2 * slots * rows * d, core, routes, weights, tokens, cot,
    )


def ordered(five, core, out, col):
    nzh, nzl = five.shape[0], five.shape[1]
    for zl in range(nzl):
        for zh in range(nzh):
            out[pl.ds((zl * nzh + zh) * OWN, OWN), pl.ds(col, LANES)] = five[zh, zl, core]


def first_kernel(core, own, gate, up, down, g5, u5, ab, bk, w_oth, wp_oth, wp_own, w_own):
    half = own.shape[1] // 2
    here = pl.ds(pl.multiple_of(core[0] * half, half), half)
    there = pl.ds(pl.multiple_of((1 - core[0]) * half, half), half)
    for k, (w, five) in enumerate(((gate, g5), (up, u5))):
        w_own[:, pl.ds(k * LANES, LANES)] = w[here, :]
        w_oth[:, pl.ds(k * LANES, LANES)] = w[there, :]
        ordered(five, core[0], wp_own, k * LANES)
        ordered(five, 1 - core[0], wp_oth, k * LANES)
    ab[...] = dot(own[:, pl.ds(0, half)], w_own[...])
    bk[...] = dot(own[:, pl.ds(half, half)], down[:, here], 1, 1)


def first(core, own, gate, up, down, g5, u5):
    slots, d = own.shape
    pair = struct(d // 2, 2 * LANES)
    return call(
        first_kernel,
        "first_half",
        [struct(slots, 2 * LANES, dtype=F32), struct(slots, LANES, dtype=F32), pair, pair, pair],
        [pltpu.VMEM(pair.shape, BF)], 20, 3 * slots * d * LANES, core, own, gate, up, down, g5, u5,
    )


def second_kernel(core, oth, down, ab, bk, w_oth, wp_oth, hid, dd, dx, rt, acc, acc2, *, block):
    slots, half = oth.shape[0], oth.shape[1] // 2
    there = pl.ds(pl.multiple_of((1 - core[0]) * half, half), half)
    acc[...] = ab[...] + dot(oth[:, pl.ds(0, half)], w_oth[...])
    acc2[...] = bk[...] + dot(oth[:, pl.ds(half, half)], down[:, there], 1, 1)
    lanes = rt.shape[1]
    for k in range(slots // block):
        at = pl.ds(k * block, block)
        a, b = acc[at, pl.ds(0, LANES)], acc[at, pl.ds(LANES, LANES)]
        back = acc2[at, :]
        s = jax.nn.sigmoid(a)
        act = a * s
        hidden = (act * b).astype(BF)
        hid[at, :] = hidden
        dd[at, pl.ds(0, LANES)] = (back * b * s * (1.0 + a * (1.0 - s))).astype(BF)
        dd[at, pl.ds(LANES, LANES)] = (back * act).astype(BF)
        route = jnp.sum((hidden.astype(F32) * back).T, axis=0, keepdims=True)
        route = padded(route, lanes)
        rt[pl.ds(k * 8, 8), :] = stacked([route], 8)
        last = slots + 8 * k
        dx[pl.ds(last, 8), pl.ds(0, lanes)] = stacked(split(route), 8).astype(BF)
        if half > lanes:
            dx[pl.ds(last, 8), pl.ds(lanes, half - lanes)] = jnp.zeros((8, half - lanes), BF)
    dx[pl.ds(0, slots), :] = dot(dd[...], wp_oth[...], 1, 1).astype(BF)


def second(core, oth, down, ab, bk, w_oth, wp_oth, block):
    slots, d = oth.shape
    half = d // 2
    steps = slots // block
    lanes = -(-block // LANES) * LANES
    return call(
        functools.partial(second_kernel, block=block),
        "second_half",
        [
            struct(slots, LANES),
            struct(slots, 2 * LANES),
            struct(slots + 8 * steps, half),
            struct(steps * 8, lanes, dtype=F32),
        ],
        [pltpu.VMEM((slots, 2 * LANES), F32), pltpu.VMEM((slots, LANES), F32)],
        20, 5 * slots * d * LANES, core, oth, down, ab, bk, w_oth, wp_oth,
    )


def mine_kernel(core, dd, wp_own, out):
    out[...] = dot(dd[...], wp_own[...], 1, 1).astype(BF)


def mine(core, dd, wp_own):
    slots, half = dd.shape[0], wp_own.shape[0]
    return call(
        mine_kernel, "own_rows", [struct(slots, half)], [], 12, 4 * slots * half * LANES,
        core, dd, wp_own,
    )[0]


def grads_kernel(core, own, oth, hid, dd, gg, gu, gd):
    half = own.shape[1] // 2
    for k, src in enumerate((own, oth)):
        base = (core[0] if k == 0 else 1 - core[0]) * half
        at = pl.ds(pl.multiple_of(base, half), half)
        both = dot(src[:, pl.ds(0, half)], dd[...], 0, 0)
        gg[at, :] = both[:, :LANES].astype(BF)
        gu[at, :] = both[:, LANES:].astype(BF)
        gd[:, at] = dot(hid[...], src[:, pl.ds(half, half)], 0, 0).astype(BF)


def grads(core, own, oth, hid, dd):
    slots, d = own.shape
    return call(
        grads_kernel,
        "weight_grads",
        [struct(d, LANES), struct(d, LANES), struct(LANES, d)],
        [], 20, 6 * slots * d * LANES, core, own, oth, hid, dd,
    )


def merge_kernel(core, got, own, rt, out, *, cap, block, nzl):
    slots, half = own.shape
    lanes = rt.shape[1]
    per = half // nzl // LANES
    for i in range(slots // block):
        tail = got[pl.ds(slots + 8 * i, 8), pl.ds(0, lanes)].astype(F32)
        route = rt[pl.ds(8 * i, 1), :] + tail[0:1] + tail[1:2]
        for j in range(block // cap):
            b = i * (block // cap) + j
            at = pl.ds(b * cap, cap)
            ends = stacked(split(padded(route[:, j * cap : (j + 1) * cap], LANES)), 8).astype(BF)
            total = (got[at, :].astype(F32) + own[at, :].astype(F32)).astype(BF)
            for zl in range(nzl):
                for q in range(per):
                    k = zl * per + q
                    out[b * nzl + zl, pl.ds(q * cap, cap), :] = total[:, k * LANES : (k + 1) * LANES]
                out[b * nzl + zl, pl.ds(per * cap, 8), :] = ends


def merge(core, got, own, rt, nzl, cap, block):
    slots, half = own.shape
    tall = half // nzl // LANES * cap + 8
    return call(
        functools.partial(merge_kernel, cap=cap, block=block, nzl=nzl),
        "merge", [struct(slots // cap * nzl, tall, LANES)], [], 12, 2 * slots * half,
        core, got, own, rt,
    )[0]


def combine_kernel(routes, weights, sel, got, out, part, *, experts, cap, nzl):
    rows = routes.shape[1]
    per = (got.shape[1] - 8) // cap
    s = sel[...]
    total = None
    for zl in range(nzl):
        for e in range(experts):
            for q in range(per):
                part[zl, pl.ds(e * cap, cap), pl.ds(q * LANES, LANES)] = got[
                    e * nzl + zl, pl.ds(q * cap, cap), :
                ]
        one = dot(s, part[zl], 0, 0)
        total = one if total is None else total + one
    total = total.astype(BF)
    mid = rows // 2
    for k in range(out.shape[0]):
        out[k, pl.ds(0, mid), :] = jnp.concatenate(
            [total[:mid, k * OWN : (k + 1) * OWN], total[mid:, k * OWN : (k + 1) * OWN]], axis=1
        )
    lines = []
    for e in range(experts):
        line = jnp.zeros((1, LANES), F32)
        for zl in range(nzl):
            tail = got[e * nzl + zl, pl.ds(per * cap, 8), :].astype(F32)
            line = line + tail[0:1] + tail[1:2]
        lines.append(line)
    r_hi, r_lo = split(stacked(lines, max(experts, 8)))
    first, second, rank = ranks(routes[...], experts)
    slot = lax.broadcasted_iota(jnp.int32, (LANES, rows), 0).astype(F32)
    ends = []
    wide = -(-rows // LANES) * LANES
    for ch, hit in enumerate((first, second)):
        place = jnp.sum(jnp.where(hit, rank, 0.0), axis=0, keepdims=True)
        pick = jnp.where(slot == place, 1.0, 0.0).astype(BF)
        value = (dot(r_hi, pick) + dot(r_lo, pick))[:experts]
        value = jnp.sum(jnp.where(hit, value, 0.0), axis=0, keepdims=True)
        w = weights[...][ch : ch + 1].astype(BF).astype(F32)
        for piece in split(padded(value / w, wide) if wide > rows else value / w):
            for k in range(wide // LANES):
                ends.append(piece[:, k * LANES : (k + 1) * LANES])
    ends = stacked(ends, 8).astype(BF)
    for k in range(out.shape[0]):
        out[k, pl.ds(mid, 8), :] = ends


def combine(routes, weights, sel, got, experts, cap, nzh, nzl):
    rows = routes.shape[1]
    per = (got.shape[1] - 8) // cap
    return pl.pallas_call(
        functools.partial(combine_kernel, experts=experts, cap=cap, nzl=nzl),
        out_shape=jax.ShapeDtypeStruct((nzh, rows // 2 + 8, LANES), BF),
        in_specs=vmem(4),
        out_specs=vmem(1)[0],
        scratch_shapes=[pltpu.VMEM((nzl, experts * cap, per * LANES), BF)],
        compiler_params=pltpu.CompilerParams(vmem_limit_bytes=16 << 20),
        name="combine",
    )(routes, weights, sel, got)


def finish_kernel(got, grad, route):
    rows = grad.shape[1]
    total = got[0].astype(F32)
    for k in range(1, got.shape[0]):
        total = total + got[k].astype(F32)
    mid = rows // 2
    turned = total[:mid].T
    grad[...] = jnp.concatenate([turned[:OWN], turned[OWN:]], axis=1).astype(BF)
    ends = total[mid:]
    n = -(-rows // LANES)
    for ch in range(2):
        pieces = [
            ends[2 * n * ch + k : 2 * n * ch + k + 1] + ends[2 * n * ch + n + k : 2 * n * ch + n + k + 1]
            for k in range(n)
        ]
        line = jnp.concatenate(pieces, axis=1) if n > 1 else pieces[0]
        route[pl.ds(ch, 1), :] = line[:, :rows]


def finish(got, rows):
    return pl.pallas_call(
        finish_kernel,
        out_shape=[
            jax.ShapeDtypeStruct((OWN, rows), BF),
            jax.ShapeDtypeStruct((2, rows), F32),
        ],
        in_specs=vmem(1),
        out_specs=vmem(2),
        compiler_params=pltpu.CompilerParams(vmem_limit_bytes=8 << 20),
        name="finish",
    )(got)


def shards(tokens, cotangent, routes, route_weight, gate_weight, up_weight, down_weight):
    rows, d = tokens.shape
    experts = lax.axis_size("ep")
    nzh, nzl = lax.axis_size("zh"), lax.axis_size("zl")
    cap = 2 * rows * routes.shape[1] // experts
    slots = experts * cap
    block = min(4, experts, d // 2 // cap) * cap
    core = lax.axis_index("core").astype(jnp.int32).reshape(1)
    routes_t, weight_t = routes.T, route_weight.T
    gate, up, down = gate_weight[0], up_weight[0], down_weight[0]
    swap = [(0, 1), (1, 0)]

    g5 = gate.reshape(nzh, nzl, 2, OWN, LANES)
    u5 = up.reshape(nzh, nzl, 2, OWN, LANES)
    packed, sel = pack(core, routes_t, weight_t, tokens, cotangent, experts, cap)
    own = lax.all_to_all(packed.reshape(experts, cap, d), "ep", 0, 0, tiled=True).reshape(slots, d)
    oth = lax.ppermute(own, "core", swap)
    ab, bk, w_oth, wp_oth, wp_own = first(core, own, gate, up, down, g5, u5)
    hid, dd, dx, rt = second(core, oth, down, ab, bk, w_oth, wp_oth, block)
    got = lax.ppermute(dx, "core", swap)
    own_rows = mine(core, dd, wp_own)
    gg, gu, gd = grads(core, own, oth, hid, dd)
    message = merge(core, got, own_rows, rt, nzl, cap, block)
    back = lax.all_to_all(message, ("ep", "zl"), 0, 0, tiled=True)
    partial = combine(routes_t, weight_t, sel, back, experts, cap, nzh, nzl)
    last = lax.all_to_all(partial, "zh", 0, 0, tiled=True)
    grad_t, route_t = finish(last, rows)
    return grad_t.T, route_t.T, gg[None], gu[None], gd[None]


def solution(mesh):
    devices = mesh.devices
    ep = devices.shape[0]
    finer = Mesh(devices.reshape(ep, -1, 2, 2), ("ep", "zh", "zl", "core"))
    in_specs = (
        P("ep", None),
        P("ep", None),
        P("ep", None),
        P("ep", None),
        P("ep", None, TP),
        P("ep", None, TP),
        P("ep", TP, None),
    )
    out_specs = (
        P("ep", TP),
        P("ep", None),
        P("ep", None, TP),
        P("ep", None, TP),
        P("ep", TP, None),
    )
    return jax.shard_map(
        shards, mesh=finer, in_specs=in_specs, out_specs=out_specs, check_vma=False
    )
```

```python
import functools

import jax
import jax.numpy as jnp
from jax import lax
from jax.experimental import pallas as pl
from jax.experimental.pallas import tpu as pltpu
from jax.sharding import Mesh
from jax.sharding import PartitionSpec as P


BF = jnp.bfloat16
F32 = jnp.float32
TP = ("zh", "zl", "core")
LANES = 128
OWN = 64


def dot(a, b, ca=1, cb=0):
    return lax.dot_general(a, b, (((ca,), (cb,)), ((), ())), preferred_element_type=F32)


def split(v):
    hi = v.astype(BF)
    return hi, (v - hi.astype(F32)).astype(BF)


def padded(v, width):
    return jnp.concatenate([v, jnp.zeros((v.shape[0], width - v.shape[1]), v.dtype)], axis=1)


def stacked(rows, height):
    place = lax.broadcasted_iota(jnp.int32, (height, rows[0].shape[1]), 0)
    out = jnp.zeros(place.shape, F32)
    for k, row in enumerate(rows):
        out = jnp.where(place == k, row.astype(F32), out)
    return out


def ranks(routes, experts):
    rows = routes.shape[1]
    ids = lax.broadcasted_iota(jnp.int32, (experts, rows), 0)
    first, second = routes[0:1] == ids, routes[1:2] == ids
    named = first | second
    before = lax.broadcasted_iota(jnp.int32, (rows, rows), 0) < lax.broadcasted_iota(
        jnp.int32, (rows, rows), 1
    )
    one, zero = jnp.ones((), F32), jnp.zeros((), F32)
    count = dot(jnp.where(named, one, zero).astype(BF), jnp.where(before, one, zero).astype(BF))
    return first, second, jnp.where(named, count, -one)


def vmem(n):
    return [pl.BlockSpec(memory_space=pltpu.VMEM)] * n


def call(kernel, out, scratch, limit, flops, *args, space=pltpu.VMEM):
    return pl.pallas_call(
        kernel,
        in_specs=[pl.BlockSpec(memory_space=pltpu.SMEM)]
        + [pl.BlockSpec(memory_space=space)] * (len(args) - 1),
        out_specs=vmem(len(out)),
        out_shape=out,
        scratch_shapes=scratch,
        compiler_params=pltpu.CompilerParams(vmem_limit_bytes=limit << 20),
        cost_estimate=pl.CostEstimate(flops=flops, bytes_accessed=flops // 400, transcendentals=0),
    )(args[0], *[pltpu.with_memory_space_constraint(a, space) if space == pltpu.HBM else a for a in args[1:]])


def struct(*shape, dtype=BF):
    return jax.ShapeDtypeStruct(shape, dtype)


def loads(pairs, sems):
    copies = [pltpu.make_async_copy(src, dst, sems.at[k]) for k, (src, dst) in enumerate(pairs)]
    for copy in copies:
        copy.start()
    return copies


def gather_lanes(x, core, nzl, out, col):
    n = x.shape[1] // LANES // nzl // 2
    for own in range(2):

        @pl.when(core == own)
        def _():
            for zl in range(nzl):
                for q in range(n):
                    at = [((2 * q + k) * nzl + zl) * LANES + own * OWN for k in range(2)]
                    pair = [x[:, pl.ds(p, OWN)] for p in at]
                    out[:, pl.ds(col + (zl * n + q) * LANES, LANES)] = jnp.concatenate(pair, axis=1)


def blocks(core, nzh, nzl):
    for zl in range(nzl):
        for zh in range(nzh):
            yield pl.ds((zl * nzh + zh) * OWN, OWN), pl.ds(
                pl.multiple_of(((zh * nzl + zl) * 2 + core) * OWN, OWN), OWN
            )


def prepare_kernel(core, routes_h, weights_h, gate_h, up_h, down_h, x_h, c_h,
                   xo, sel, wsel, w_own, w_oth,
                   routes, weights, gate, up, down, x, c, turned, sems,
                   *, experts, cap, nzh, nzl):
    half = x.shape[1] // 2
    copies = loads(
        (
            (routes_h, routes),
            (weights_h, weights),
            (gate_h, gate),
            (up_h, up),
            (down_h, down),
            (x_h, x),
            (c_h, c),
        ),
        sems,
    )
    copies[0].wait()
    copies[1].wait()
    first, second, rank = ranks(routes[...], experts)
    w = weights[...]
    mine = jnp.where(first, w[0:1], 0.0) + jnp.where(second, w[1:2], 0.0)
    slot = lax.broadcasted_iota(jnp.int32, (cap, rank.shape[1]), 0).astype(F32)
    for e in range(experts):
        hit = rank[e : e + 1] == slot
        sel[pl.ds(e * cap, cap), :] = jnp.where(hit, 1.0, 0.0).astype(BF)
        wsel[pl.ds(e * cap, cap), :] = jnp.where(hit, mine[e : e + 1], 0.0).astype(BF)
    for k, src in enumerate((gate, up, turned)):
        copies[2 + k].wait()
        if k == 2:
            turned[...] = down[...].T
        for to_ref, who in ((w_own, core[0]), (w_oth, 1 - core[0])):
            for to, at in blocks(who, nzh, nzl):
                to_ref[to, pl.ds(k * LANES, LANES)] = src[at, :]
    copies[5].wait()
    gather_lanes(x, core[0], nzl, xo, 0)
    copies[6].wait()
    gather_lanes(c, core[0], nzl, xo, half)


def prepare(core, routes, weights, gate, up, down, tokens, cot, experts, cap, nzh, nzl):
    rows, d = tokens.shape
    slots = experts * cap
    return call(
        functools.partial(prepare_kernel, experts=experts, cap=cap, nzh=nzh, nzl=nzl),
        [struct(rows, d)] + [struct(slots, rows)] * 2 + [struct(d // 2, 3 * LANES)] * 2,
        [
            pltpu.VMEM(routes.shape, jnp.int32),
            pltpu.VMEM(weights.shape, F32),
            pltpu.VMEM((d, LANES), BF),
            pltpu.VMEM((d, LANES), BF),
            pltpu.VMEM((LANES, d), BF),
            pltpu.VMEM((rows, d), BF),
            pltpu.VMEM((rows, d), BF),
            pltpu.VMEM((d, LANES), BF),
            pltpu.SemaphoreType.DMA((7,)),
        ],
        20, 2 * slots * rows * d, core, routes, weights, gate, up, down, tokens, cot,
        space=pltpu.HBM,
    )


def pack_kernel(core, xo, sel, wsel, out):
    half = xo.shape[1] // 2
    out[:, pl.ds(0, half)] = dot(sel[...], xo[:, pl.ds(0, half)]).astype(BF)
    out[:, pl.ds(half, half)] = dot(wsel[...], xo[:, pl.ds(half, half)]).astype(BF)


def pack(core, xo, sel, wsel):
    slots, (rows, d) = sel.shape[0], xo.shape
    return call(
        pack_kernel, [struct(slots, d)], [], 12, 2 * slots * rows * d, core, xo, sel, wsel
    )[0]


def forward_kernel(core, own, w_own, w_got, out):
    half = own.shape[1] // 2
    for k, w in enumerate((w_own, w_got)):
        col = 3 * LANES * k
        out[:, pl.ds(col, 2 * LANES)] = dot(own[:, pl.ds(0, half)], w[:, pl.ds(0, 2 * LANES)]).astype(BF)
    down = jnp.concatenate([w[:, pl.ds(2 * LANES, LANES)] for w in (w_own, w_got)], axis=1)
    back = dot(own[:, pl.ds(half, half)], down).astype(BF)
    out[:, pl.ds(2 * LANES, LANES)] = back[:, :LANES]
    out[:, pl.ds(5 * LANES, LANES)] = back[:, LANES:]


def forward(core, own, w_own, w_got):
    slots, d = own.shape
    return call(
        forward_kernel, [struct(slots, 6 * LANES)], [], 20, 6 * slots * d * LANES,
        core, own, w_own, w_got,
    )[0]


def backward_kernel(core, part, got, w_own, w_got, hid, dd, out, *, cap, nzl):
    slots = part.shape[0]
    half = w_own.shape[0]
    per = half // nzl // LANES
    lane = 3 * LANES
    group = slots // 4 if slots % (4 * cap) == 0 else slots
    for i in range(slots // group):
        at = pl.ds(i * group, group)
        route = None
        for k in range(2):

            def total(j):
                cols = [pl.ds(lane * side + LANES * j, LANES) for side in (k, 1 - k)]
                return part[at, cols[0]].astype(F32) + got[at, cols[1]].astype(F32)

            a, b, back = total(0), total(1), total(2)
            s = jax.nn.sigmoid(a)
            act = a * s
            hidden = (act * b).astype(BF)
            hid[at, pl.ds(k * LANES, LANES)] = hidden
            dd[at, pl.ds(2 * k * LANES, LANES)] = (back * b * s * (1.0 + a * (1.0 - s))).astype(BF)
            dd[at, pl.ds((2 * k + 1) * LANES, LANES)] = (back * act).astype(BF)
            one = jnp.sum((hidden.astype(F32) * back).T, axis=0, keepdims=True)
            route = one if route is None else route + one
        rows = dot(dd[at, pl.ds(0, 2 * LANES)], w_own[:, pl.ds(0, 2 * LANES)], 1, 1)
        rows = rows + dot(dd[at, pl.ds(2 * LANES, 2 * LANES)], w_got[:, pl.ds(0, 2 * LANES)], 1, 1)
        rows = rows.astype(BF)
        for j in range(group // cap):
            b = i * (group // cap) + j
            ends = stacked(split(padded(route[:, j * cap : (j + 1) * cap], LANES)), 8).astype(BF)
            for zl in range(nzl):
                for q in range(per):
                    k = zl * per + q
                    out[b * nzl + zl, pl.ds(q * cap, cap), :] = rows[
                        j * cap : (j + 1) * cap, k * LANES : (k + 1) * LANES
                    ]
                out[b * nzl + zl, pl.ds(per * cap, 8), :] = ends


def backward(core, part, got, w_own, w_got, nzl, cap):
    slots, half = part.shape[0], w_own.shape[0]
    tall = half // nzl // LANES * cap + 8
    return call(
        functools.partial(backward_kernel, cap=cap, nzl=nzl),
        [
            struct(slots, 2 * LANES),
            struct(slots, 4 * LANES),
            struct(slots // cap * nzl, tall, LANES),
        ],
        [], 24, 8 * slots * half * LANES, core, part, got, w_own, w_got,
    )


def grads_kernel(core, own, hid, dd, keep, send):
    half = own.shape[1] // 2
    both = dot(own[:, pl.ds(0, half)], dd[...], 0, 0)
    keep[:, pl.ds(0, 2 * LANES)] = both[:, : 2 * LANES].astype(BF)
    send[:, pl.ds(0, 2 * LANES)] = both[:, 2 * LANES :].astype(BF)
    down = dot(own[:, pl.ds(half, half)], hid[...], 0, 0)
    keep[:, pl.ds(2 * LANES, LANES)] = down[:, :LANES].astype(BF)
    send[:, pl.ds(2 * LANES, LANES)] = down[:, LANES:].astype(BF)


def grads(core, own, hid, dd):
    slots, d = own.shape
    return call(
        grads_kernel, [struct(d // 2, 3 * LANES)] * 2, [], 24,
        6 * slots * d * LANES, core, own, hid, dd,
    )


def place_kernel(core, keep, got, gg, gu, gd, turned, *, nzh, nzl):
    for k, out in enumerate((gg, gu, turned)):
        for src, who in ((keep, core[0]), (got, 1 - core[0])):
            for at, to in blocks(who, nzh, nzl):
                out[to, :] = src[at, pl.ds(k * LANES, LANES)]
    gd[...] = turned[...].T


def place(core, keep, got, nzh, nzl):
    d = 2 * keep.shape[0]
    return call(
        functools.partial(place_kernel, nzh=nzh, nzl=nzl),
        [struct(d, LANES), struct(d, LANES), struct(LANES, d)],
        [pltpu.VMEM((d, LANES), BF)],
        12, 1 << 28, core, keep, got,
    )


def combine_kernel(routes, weights, sel, got, out, part, *, experts, cap, nzl):
    rows = routes.shape[1]
    per = (got.shape[1] - 8) // cap
    s = sel[...]
    total = None
    for zl in range(nzl):
        for e in range(experts):
            for q in range(per):
                part[zl, pl.ds(e * cap, cap), pl.ds(q * LANES, LANES)] = got[
                    e * nzl + zl, pl.ds(q * cap, cap), :
                ]
        one = dot(s, part[zl], 0, 0)
        total = one if total is None else total + one
    total = total.astype(BF)
    mid = rows // 2
    for k in range(out.shape[0]):
        out[k, pl.ds(0, mid), :] = jnp.concatenate(
            [total[:mid, k * OWN : (k + 1) * OWN], total[mid:, k * OWN : (k + 1) * OWN]], axis=1
        )
    lines = []
    for e in range(experts):
        line = jnp.zeros((1, LANES), F32)
        for zl in range(nzl):
            tail = got[e * nzl + zl, pl.ds(per * cap, 8), :].astype(F32)
            line = line + tail[0:1] + tail[1:2]
        lines.append(line)
    r_hi, r_lo = split(stacked(lines, max(experts, 8)))
    first, second, rank = ranks(routes[...], experts)
    slot = lax.broadcasted_iota(jnp.int32, (LANES, rows), 0).astype(F32)
    ends = []
    wide = -(-rows // LANES) * LANES
    for ch, hit in enumerate((first, second)):
        place = jnp.sum(jnp.where(hit, rank, 0.0), axis=0, keepdims=True)
        pick = jnp.where(slot == place, 1.0, 0.0).astype(BF)
        value = (dot(r_hi, pick) + dot(r_lo, pick))[:experts]
        value = jnp.sum(jnp.where(hit, value, 0.0), axis=0, keepdims=True)
        w = weights[...][ch : ch + 1].astype(BF).astype(F32)
        for piece in split(padded(value / w, wide) if wide > rows else value / w):
            for k in range(wide // LANES):
                ends.append(piece[:, k * LANES : (k + 1) * LANES])
    ends = stacked(ends, 8).astype(BF)
    for k in range(out.shape[0]):
        out[k, pl.ds(mid, 8), :] = ends


def combine(routes, weights, sel, got, experts, cap, nzh, nzl):
    rows = routes.shape[1]
    per = (got.shape[1] - 8) // cap
    return pl.pallas_call(
        functools.partial(combine_kernel, experts=experts, cap=cap, nzl=nzl),
        out_shape=jax.ShapeDtypeStruct((nzh, rows // 2 + 8, LANES), BF),
        in_specs=vmem(4),
        out_specs=vmem(1)[0],
        scratch_shapes=[pltpu.VMEM((nzl, experts * cap, per * LANES), BF)],
        compiler_params=pltpu.CompilerParams(vmem_limit_bytes=16 << 20),
        name="combine",
    )(routes, weights, sel, got)


def finish_kernel(got, grad, route):
    rows = grad.shape[1]
    total = got[0].astype(F32)
    for k in range(1, got.shape[0]):
        total = total + got[k].astype(F32)
    mid = rows // 2
    turned = total[:mid].T
    grad[...] = jnp.concatenate([turned[:OWN], turned[OWN:]], axis=1).astype(BF)
    ends = total[mid:]
    n = -(-rows // LANES)
    for ch in range(2):
        pieces = [
            ends[2 * n * ch + k : 2 * n * ch + k + 1] + ends[2 * n * ch + n + k : 2 * n * ch + n + k + 1]
            for k in range(n)
        ]
        line = jnp.concatenate(pieces, axis=1) if n > 1 else pieces[0]
        route[pl.ds(ch, 1), :] = line[:, :rows]


def finish(got, rows):
    return pl.pallas_call(
        finish_kernel,
        out_shape=[
            jax.ShapeDtypeStruct((OWN, rows), BF),
            jax.ShapeDtypeStruct((2, rows), F32),
        ],
        in_specs=vmem(1),
        out_specs=vmem(2),
        compiler_params=pltpu.CompilerParams(vmem_limit_bytes=8 << 20),
        name="finish",
    )(got)


def shards(tokens, cotangent, routes, route_weight, gate_weight, up_weight, down_weight):
    rows, d = tokens.shape
    experts = lax.axis_size("ep")
    nzh, nzl = lax.axis_size("zh"), lax.axis_size("zl")
    cap = 2 * rows * routes.shape[1] // experts
    slots = experts * cap
    core = lax.axis_index("core").astype(jnp.int32).reshape(1)
    routes_t, weight_t = routes.T, route_weight.T
    gate, up, down = gate_weight[0], up_weight[0], down_weight[0]
    swap = [(0, 1), (1, 0)]

    xo, sel, wsel, w_own, w_oth = prepare(
        core, routes_t, weight_t, gate, up, down, tokens, cotangent, experts, cap, nzh, nzl
    )
    w_got = lax.ppermute(w_oth, "core", swap)
    packed = pack(core, xo, sel, wsel)
    packed, w_own, w_got = lax.optimization_barrier((packed, w_own, w_got))
    own = lax.all_to_all(packed.reshape(experts, cap, d), "ep", 0, 0, tiled=True).reshape(slots, d)
    part = forward(core, own, w_own, w_got)
    got = lax.ppermute(part, "core", swap)
    hid, dd, message = backward(core, part, got, w_own, w_got, nzl, cap)
    keep, send = grads(core, own, hid, dd)
    moved = lax.ppermute(send, "core", swap)
    gg, gu, gd = place(core, keep, moved, nzh, nzl)
    back = lax.all_to_all(message, ("ep", "zl"), 0, 0, tiled=True)
    partial = combine(routes_t, weight_t, sel, back, experts, cap, nzh, nzl)
    last = lax.all_to_all(partial, "zh", 0, 0, tiled=True)
    grad_t, route_t = finish(last, rows)
    return grad_t.T, route_t.T, gg[None], gu[None], gd[None]


def solution(mesh):
    devices = mesh.devices
    ep = devices.shape[0]
    finer = Mesh(devices.reshape(ep, -1, 2, 2), ("ep", "zh", "zl", "core"))
    in_specs = (
        P("ep", None),
        P("ep", None),
        P("ep", None),
        P("ep", None),
        P("ep", None, TP),
        P("ep", None, TP),
        P("ep", TP, None),
    )
    out_specs = (
        P("ep", TP),
        P("ep", None),
        P("ep", None, TP),
        P("ep", None, TP),
        P("ep", TP, None),
    )
    return jax.shard_map(
        shards, mesh=finer, in_specs=in_specs, out_specs=out_specs, check_vma=False
    )
```

```python
import functools

import jax
import jax.numpy as jnp
from jax import lax
from jax.experimental import pallas as pl
from jax.experimental.pallas import tpu as pltpu
from jax.sharding import Mesh
from jax.sharding import PartitionSpec as P


BF = jnp.bfloat16
F32 = jnp.float32
TP = ("zh", "zl", "core")
LANES = 128
OWN = 64


def dot(a, b, ca=1, cb=0):
    return lax.dot_general(a, b, (((ca,), (cb,)), ((), ())), preferred_element_type=F32)


def split(v):
    hi = v.astype(BF)
    return hi, (v - hi.astype(F32)).astype(BF)


def padded(v, width):
    return jnp.concatenate([v, jnp.zeros((v.shape[0], width - v.shape[1]), v.dtype)], axis=1)


def stacked(rows, height):
    place = lax.broadcasted_iota(jnp.int32, (height, rows[0].shape[1]), 0)
    out = jnp.zeros(place.shape, F32)
    for k, row in enumerate(rows):
        out = jnp.where(place == k, row.astype(F32), out)
    return out


def ranks(routes, experts):
    rows = routes.shape[1]
    ids = lax.broadcasted_iota(jnp.int32, (experts, rows), 0)
    first, second = routes[0:1] == ids, routes[1:2] == ids
    named = first | second
    before = lax.broadcasted_iota(jnp.int32, (rows, rows), 0) < lax.broadcasted_iota(
        jnp.int32, (rows, rows), 1
    )
    one, zero = jnp.ones((), F32), jnp.zeros((), F32)
    count = dot(jnp.where(named, one, zero).astype(BF), jnp.where(before, one, zero).astype(BF))
    return first, second, jnp.where(named, count, -one)


def vmem(n):
    return [pl.BlockSpec(memory_space=pltpu.VMEM)] * n


def call(kernel, out, scratch, limit, flops, *args, space=pltpu.VMEM):
    return pl.pallas_call(
        kernel,
        in_specs=[pl.BlockSpec(memory_space=pltpu.SMEM)]
        + [pl.BlockSpec(memory_space=space)] * (len(args) - 1),
        out_specs=vmem(len(out)),
        out_shape=out,
        scratch_shapes=scratch,
        compiler_params=pltpu.CompilerParams(vmem_limit_bytes=limit << 20),
        cost_estimate=pl.CostEstimate(flops=flops, bytes_accessed=flops // 400, transcendentals=0),
    )(args[0], *[pltpu.with_memory_space_constraint(a, space) if space == pltpu.HBM else a for a in args[1:]])


def struct(*shape, dtype=BF):
    return jax.ShapeDtypeStruct(shape, dtype)


def loads(pairs, sems):
    copies = [pltpu.make_async_copy(src, dst, sems.at[k]) for k, (src, dst) in enumerate(pairs)]
    for copy in copies:
        copy.start()
    return copies


def gather_lanes(x, core, nzl, out, col):
    n = x.shape[1] // LANES // nzl // 2
    for own in range(2):

        @pl.when(core == own)
        def _():
            for zl in range(nzl):
                for q in range(n):
                    at = [((2 * q + k) * nzl + zl) * LANES + own * OWN for k in range(2)]
                    pair = [x[:, pl.ds(p, OWN)] for p in at]
                    out[:, pl.ds(col + (zl * n + q) * LANES, LANES)] = jnp.concatenate(pair, axis=1)


def blocks(core, nzh, nzl):
    for zl in range(nzl):
        for zh in range(nzh):
            yield pl.ds((zl * nzh + zh) * OWN, OWN), pl.ds(
                pl.multiple_of(((zh * nzl + zl) * 2 + core) * OWN, OWN), OWN
            )


def prepare_kernel(core, routes_h, weights_h, gate_h, up_h, down_h, x_h, c_h,
                   routes, weights, x, c, w_own, w_oth,
                   gate, up, down, turned, sems, *, nzh, nzl):
    copies = loads(
        (
            (gate_h, gate),
            (up_h, up),
            (down_h, down),
            (routes_h, routes),
            (weights_h, weights),
            (x_h, x),
            (c_h, c),
        ),
        sems,
    )
    for k, src in enumerate((gate, up, turned)):
        copies[k].wait()
        if k == 2:
            turned[...] = down[...].T
        for to_ref, who in ((w_oth, 1 - core[0]), (w_own, core[0])):
            for to, at in blocks(who, nzh, nzl):
                to_ref[to, pl.ds(k * LANES, LANES)] = src[at, :]
    for copy in copies[3:]:
        copy.wait()


def prepare(core, routes, weights, gate, up, down, tokens, cot, nzh, nzl):
    rows, d = tokens.shape
    return call(
        functools.partial(prepare_kernel, nzh=nzh, nzl=nzl),
        [struct(*routes.shape, dtype=jnp.int32), struct(*weights.shape, dtype=F32)]
        + [struct(rows, d)] * 2
        + [struct(d // 2, 3 * LANES)] * 2,
        [
            pltpu.VMEM((d, LANES), BF),
            pltpu.VMEM((d, LANES), BF),
            pltpu.VMEM((LANES, d), BF),
            pltpu.VMEM((d, LANES), BF),
            pltpu.SemaphoreType.DMA((7,)),
        ],
        16, 1 << 28, core, routes, weights, gate, up, down, tokens, cot, space=pltpu.HBM,
    )


def pack_kernel(core, routes, weights, x, c, out, sel, xo, wsel, *, experts, cap, nzl):
    half = x.shape[1] // 2
    first, second, rank = ranks(routes[...], experts)
    w = weights[...]
    mine = jnp.where(first, w[0:1], 0.0) + jnp.where(second, w[1:2], 0.0)
    slot = lax.broadcasted_iota(jnp.int32, (cap, rank.shape[1]), 0).astype(F32)
    for e in range(experts):
        hit = rank[e : e + 1] == slot
        sel[pl.ds(e * cap, cap), :] = jnp.where(hit, 1.0, 0.0).astype(BF)
        wsel[pl.ds(e * cap, cap), :] = jnp.where(hit, mine[e : e + 1], 0.0).astype(BF)
    gather_lanes(x, core[0], nzl, xo, 0)
    gather_lanes(c, core[0], nzl, xo, half)
    out[:, pl.ds(0, half)] = dot(sel[...], xo[:, pl.ds(0, half)]).astype(BF)
    out[:, pl.ds(half, half)] = dot(wsel[...], xo[:, pl.ds(half, half)]).astype(BF)


def pack(core, routes, weights, x, c, experts, cap, nzl):
    rows, d = x.shape
    slots = experts * cap
    return call(
        functools.partial(pack_kernel, experts=experts, cap=cap, nzl=nzl),
        [struct(slots, d), struct(slots, rows)],
        [pltpu.VMEM((rows, d), BF), pltpu.VMEM((slots, rows), BF)],
        12, 2 * slots * rows * d, core, routes, weights, x, c,
    )


def forward_kernel(core, own, w_own, w_got, out):
    half = own.shape[1] // 2
    for k, w in enumerate((w_own, w_got)):
        col = 3 * LANES * k
        out[:, pl.ds(col, 2 * LANES)] = dot(own[:, pl.ds(0, half)], w[:, pl.ds(0, 2 * LANES)]).astype(BF)
    down = jnp.concatenate([w[:, pl.ds(2 * LANES, LANES)] for w in (w_own, w_got)], axis=1)
    back = dot(own[:, pl.ds(half, half)], down).astype(BF)
    out[:, pl.ds(2 * LANES, LANES)] = back[:, :LANES]
    out[:, pl.ds(5 * LANES, LANES)] = back[:, LANES:]


def forward(core, own, w_own, w_got):
    slots, d = own.shape
    return call(
        forward_kernel, [struct(slots, 6 * LANES)], [], 20, 6 * slots * d * LANES,
        core, own, w_own, w_got,
    )[0]


def backward_kernel(core, part, got, w_own, w_got, hid, dd, out, *, cap, nzl):
    slots = part.shape[0]
    half = w_own.shape[0]
    per = half // nzl // LANES
    lane = 3 * LANES
    group = slots // 2 if slots % (2 * cap) == 0 else slots
    for i in range(slots // group):
        at = pl.ds(i * group, group)
        route = None
        for k in range(2):

            def total(j):
                cols = [pl.ds(lane * side + LANES * j, LANES) for side in (k, 1 - k)]
                return part[at, cols[0]].astype(F32) + got[at, cols[1]].astype(F32)

            a, b, back = total(0), total(1), total(2)
            s = jax.nn.sigmoid(a)
            act = a * s
            hidden = (act * b).astype(BF)
            hid[at, pl.ds(k * LANES, LANES)] = hidden
            dd[at, pl.ds(2 * k * LANES, LANES)] = (back * b * s * (1.0 + a * (1.0 - s))).astype(BF)
            dd[at, pl.ds((2 * k + 1) * LANES, LANES)] = (back * act).astype(BF)
            one = jnp.sum((hidden.astype(F32) * back).T, axis=0, keepdims=True)
            route = one if route is None else route + one
        rows = dot(dd[at, pl.ds(0, 2 * LANES)], w_own[:, pl.ds(0, 2 * LANES)], 1, 1)
        rows = rows + dot(dd[at, pl.ds(2 * LANES, 2 * LANES)], w_got[:, pl.ds(0, 2 * LANES)], 1, 1)
        rows = rows.astype(BF)
        for j in range(group // cap):
            b = i * (group // cap) + j
            ends = stacked(split(padded(route[:, j * cap : (j + 1) * cap], LANES)), 8).astype(BF)
            for zl in range(nzl):
                for q in range(per):
                    k = zl * per + q
                    out[b * nzl + zl, pl.ds(q * cap, cap), :] = rows[
                        j * cap : (j + 1) * cap, k * LANES : (k + 1) * LANES
                    ]
                out[b * nzl + zl, pl.ds(per * cap, 8), :] = ends


def backward(core, part, got, w_own, w_got, nzl, cap):
    slots, half = part.shape[0], w_own.shape[0]
    tall = half // nzl // LANES * cap + 8
    return call(
        functools.partial(backward_kernel, cap=cap, nzl=nzl),
        [
            struct(slots, 2 * LANES),
            struct(slots, 4 * LANES),
            struct(slots // cap * nzl, tall, LANES),
        ],
        [], 24, 8 * slots * half * LANES, core, part, got, w_own, w_got,
    )


def grads_kernel(core, own, hid, dd, keep, send):
    half = own.shape[1] // 2
    both = dot(own[:, pl.ds(0, half)], dd[...], 0, 0)
    keep[:, pl.ds(0, 2 * LANES)] = both[:, : 2 * LANES].astype(BF)
    send[:, pl.ds(0, 2 * LANES)] = both[:, 2 * LANES :].astype(BF)
    down = dot(own[:, pl.ds(half, half)], hid[...], 0, 0)
    keep[:, pl.ds(2 * LANES, LANES)] = down[:, :LANES].astype(BF)
    send[:, pl.ds(2 * LANES, LANES)] = down[:, LANES:].astype(BF)


def grads(core, own, hid, dd):
    slots, d = own.shape
    return call(
        grads_kernel, [struct(d // 2, 3 * LANES)] * 2, [], 24,
        6 * slots * d * LANES, core, own, hid, dd,
    )


def place_kernel(core, keep, got, gg, gu, gd, turned, *, nzh, nzl):
    for k, out in enumerate((gg, gu, turned)):
        for src, who in ((keep, core[0]), (got, 1 - core[0])):
            for at, to in blocks(who, nzh, nzl):
                out[to, :] = src[at, pl.ds(k * LANES, LANES)]
    gd[...] = turned[...].T


def place(core, keep, got, nzh, nzl):
    d = 2 * keep.shape[0]
    return call(
        functools.partial(place_kernel, nzh=nzh, nzl=nzl),
        [struct(d, LANES), struct(d, LANES), struct(LANES, d)],
        [pltpu.VMEM((d, LANES), BF)],
        12, 1 << 28, core, keep, got,
    )


def combine_kernel(routes, weights, sel, got, out, part, *, experts, cap, nzl):
    rows = routes.shape[1]
    per = (got.shape[1] - 8) // cap
    s = sel[...]
    total = None
    for zl in range(nzl):
        for e in range(experts):
            for q in range(per):
                part[zl, pl.ds(e * cap, cap), pl.ds(q * LANES, LANES)] = got[
                    e * nzl + zl, pl.ds(q * cap, cap), :
                ]
        one = dot(s, part[zl], 0, 0)
        total = one if total is None else total + one
    total = total.astype(BF)
    mid = rows // 2
    for k in range(out.shape[0]):
        out[k, pl.ds(0, mid), :] = jnp.concatenate(
            [total[:mid, k * OWN : (k + 1) * OWN], total[mid:, k * OWN : (k + 1) * OWN]], axis=1
        )
    lines = []
    for e in range(experts):
        line = jnp.zeros((1, LANES), F32)
        for zl in range(nzl):
            tail = got[e * nzl + zl, pl.ds(per * cap, 8), :].astype(F32)
            line = line + tail[0:1] + tail[1:2]
        lines.append(line)
    r_hi, r_lo = split(stacked(lines, max(experts, 8)))
    first, second, rank = ranks(routes[...], experts)
    slot = lax.broadcasted_iota(jnp.int32, (LANES, rows), 0).astype(F32)
    ends = []
    wide = -(-rows // LANES) * LANES
    for ch, hit in enumerate((first, second)):
        place = jnp.sum(jnp.where(hit, rank, 0.0), axis=0, keepdims=True)
        pick = jnp.where(slot == place, 1.0, 0.0).astype(BF)
        value = (dot(r_hi, pick) + dot(r_lo, pick))[:experts]
        value = jnp.sum(jnp.where(hit, value, 0.0), axis=0, keepdims=True)
        w = weights[...][ch : ch + 1].astype(BF).astype(F32)
        for piece in split(padded(value / w, wide) if wide > rows else value / w):
            for k in range(wide // LANES):
                ends.append(piece[:, k * LANES : (k + 1) * LANES])
    ends = stacked(ends, 8).astype(BF)
    for k in range(out.shape[0]):
        out[k, pl.ds(mid, 8), :] = ends


def combine(routes, weights, sel, got, experts, cap, nzh, nzl):
    rows = routes.shape[1]
    per = (got.shape[1] - 8) // cap
    return pl.pallas_call(
        functools.partial(combine_kernel, experts=experts, cap=cap, nzl=nzl),
        out_shape=jax.ShapeDtypeStruct((nzh, rows // 2 + 8, LANES), BF),
        in_specs=vmem(4),
        out_specs=vmem(1)[0],
        scratch_shapes=[pltpu.VMEM((nzl, experts * cap, per * LANES), BF)],
        compiler_params=pltpu.CompilerParams(vmem_limit_bytes=16 << 20),
        name="combine",
    )(routes, weights, sel, got)


def finish_kernel(got, grad, route):
    rows = grad.shape[1]
    total = got[0].astype(F32)
    for k in range(1, got.shape[0]):
        total = total + got[k].astype(F32)
    mid = rows // 2
    turned = total[:mid].T
    grad[...] = jnp.concatenate([turned[:OWN], turned[OWN:]], axis=1).astype(BF)
    ends = total[mid:]
    n = -(-rows // LANES)
    for ch in range(2):
        pieces = [
            ends[2 * n * ch + k : 2 * n * ch + k + 1] + ends[2 * n * ch + n + k : 2 * n * ch + n + k + 1]
            for k in range(n)
        ]
        line = jnp.concatenate(pieces, axis=1) if n > 1 else pieces[0]
        route[pl.ds(ch, 1), :] = line[:, :rows]


def finish(got, rows):
    return pl.pallas_call(
        finish_kernel,
        out_shape=[
            jax.ShapeDtypeStruct((OWN, rows), BF),
            jax.ShapeDtypeStruct((2, rows), F32),
        ],
        in_specs=vmem(1),
        out_specs=vmem(2),
        compiler_params=pltpu.CompilerParams(vmem_limit_bytes=8 << 20),
        name="finish",
    )(got)


def shards(tokens, cotangent, routes, route_weight, gate_weight, up_weight, down_weight):
    rows, d = tokens.shape
    experts = lax.axis_size("ep")
    nzh, nzl = lax.axis_size("zh"), lax.axis_size("zl")
    cap = 2 * rows * routes.shape[1] // experts
    slots = experts * cap
    core = lax.axis_index("core").astype(jnp.int32).reshape(1)
    routes_t, weight_t = routes.T, route_weight.T
    gate, up, down = gate_weight[0], up_weight[0], down_weight[0]
    swap = [(0, 1), (1, 0)]

    routes_v, weight_v, x_v, c_v, w_own, w_oth = prepare(
        core, routes_t, weight_t, gate, up, down, tokens, cotangent, nzh, nzl
    )
    w_got = lax.ppermute(w_oth, "core", swap)
    packed, sel = pack(core, routes_v, weight_v, x_v, c_v, experts, cap, nzl)
    packed, w_own, w_got = lax.optimization_barrier((packed, w_own, w_got))
    own = lax.all_to_all(packed.reshape(experts, cap, d), "ep", 0, 0, tiled=True).reshape(slots, d)
    part = forward(core, own, w_own, w_got)
    got = lax.ppermute(part, "core", swap)
    hid, dd, message = backward(core, part, got, w_own, w_got, nzl, cap)
    keep, send = grads(core, own, hid, dd)
    moved = lax.ppermute(send, "core", swap)
    gg, gu, gd = place(core, keep, moved, nzh, nzl)
    back = lax.all_to_all(message, ("ep", "zl"), 0, 0, tiled=True)
    partial = combine(routes_v, weight_v, sel, back, experts, cap, nzh, nzl)
    last = lax.all_to_all(partial, "zh", 0, 0, tiled=True)
    grad_t, route_t = finish(last, rows)
    return grad_t.T, route_t.T, gg[None], gu[None], gd[None]


def solution(mesh):
    devices = mesh.devices
    ep = devices.shape[0]
    finer = Mesh(devices.reshape(ep, -1, 2, 2), ("ep", "zh", "zl", "core"))
    in_specs = (
        P("ep", None),
        P("ep", None),
        P("ep", None),
        P("ep", None),
        P("ep", None, TP),
        P("ep", None, TP),
        P("ep", TP, None),
    )
    out_specs = (
        P("ep", TP),
        P("ep", None),
        P("ep", None, TP),
        P("ep", None, TP),
        P("ep", TP, None),
    )
    return jax.shard_map(
        shards, mesh=finer, in_specs=in_specs, out_specs=out_specs, check_vma=False
    )
```

```python
import functools

import jax
import jax.numpy as jnp
from jax import lax
from jax.experimental import pallas as pl
from jax.experimental.pallas import tpu as pltpu
from jax.sharding import Mesh
from jax.sharding import PartitionSpec as P


BF = jnp.bfloat16
F32 = jnp.float32
TP = ("zh", "zl", "core")
LANES = 128
OWN = 64


def dot(a, b, ca=1, cb=0):
    return lax.dot_general(a, b, (((ca,), (cb,)), ((), ())), preferred_element_type=F32)


def split(v):
    hi = v.astype(BF)
    return hi, (v - hi.astype(F32)).astype(BF)


def padded(v, width):
    return jnp.concatenate([v, jnp.zeros((v.shape[0], width - v.shape[1]), v.dtype)], axis=1)


def stacked(rows, height):
    place = lax.broadcasted_iota(jnp.int32, (height, rows[0].shape[1]), 0)
    out = jnp.zeros(place.shape, F32)
    for k, row in enumerate(rows):
        out = jnp.where(place == k, row.astype(F32), out)
    return out


def ranks(routes, experts):
    rows = routes.shape[1]
    ids = lax.broadcasted_iota(jnp.int32, (experts, rows), 0)
    first, second = routes[0:1] == ids, routes[1:2] == ids
    named = first | second
    before = lax.broadcasted_iota(jnp.int32, (rows, rows), 0) < lax.broadcasted_iota(
        jnp.int32, (rows, rows), 1
    )
    one, zero = jnp.ones((), F32), jnp.zeros((), F32)
    count = dot(jnp.where(named, one, zero).astype(BF), jnp.where(before, one, zero).astype(BF))
    return first, second, jnp.where(named, count, -one)


def vmem(n):
    return [pl.BlockSpec(memory_space=pltpu.VMEM)] * n


def call(kernel, out, scratch, limit, flops, *args, space=pltpu.VMEM):
    return pl.pallas_call(
        kernel,
        in_specs=[pl.BlockSpec(memory_space=pltpu.SMEM)]
        + [pl.BlockSpec(memory_space=space)] * (len(args) - 1),
        out_specs=vmem(len(out)),
        out_shape=out,
        scratch_shapes=scratch,
        compiler_params=pltpu.CompilerParams(vmem_limit_bytes=limit << 20),
        cost_estimate=pl.CostEstimate(flops=flops, bytes_accessed=flops // 400, transcendentals=0),
    )(args[0], *[pltpu.with_memory_space_constraint(a, space) if space == pltpu.HBM else a for a in args[1:]])


def struct(*shape, dtype=BF):
    return jax.ShapeDtypeStruct(shape, dtype)


def loads(pairs, sems):
    copies = [pltpu.make_async_copy(src, dst, sems.at[k]) for k, (src, dst) in enumerate(pairs)]
    for copy in copies:
        copy.start()
    return copies


def gather_lanes(x, core, nzl, out, col):
    n = x.shape[1] // LANES // nzl // 2
    for own in range(2):

        @pl.when(core == own)
        def _():
            for zl in range(nzl):
                for q in range(n):
                    at = [((2 * q + k) * nzl + zl) * LANES + own * OWN for k in range(2)]
                    pair = [x[:, pl.ds(p, OWN)] for p in at]
                    out[:, pl.ds(col + (zl * n + q) * LANES, LANES)] = jnp.concatenate(pair, axis=1)


def blocks(core, nzh, nzl):
    for zl in range(nzl):
        for zh in range(nzh):
            yield pl.ds((zl * nzh + zh) * OWN, OWN), pl.ds(
                pl.multiple_of(((zh * nzl + zl) * 2 + core) * OWN, OWN), OWN
            )


def prepare_kernel(core, routes_h, weights_h, gate_h, up_h, down_h, x_h, c_h,
                   routes, weights, x, c, w_own, w_oth,
                   gate, up, down, turned, sems, *, nzh, nzl):
    copies = loads(
        (
            (gate_h, gate),
            (up_h, up),
            (down_h, down),
            (routes_h, routes),
            (weights_h, weights),
            (x_h, x),
            (c_h, c),
        ),
        sems,
    )
    for k, src in enumerate((gate, up, turned)):
        copies[k].wait()
        if k == 2:
            turned[...] = down[...].T
        for to_ref, who in ((w_oth, 1 - core[0]), (w_own, core[0])):
            for to, at in blocks(who, nzh, nzl):
                to_ref[to, pl.ds(k * LANES, LANES)] = src[at, :]
    for copy in copies[3:]:
        copy.wait()


def prepare(core, routes, weights, gate, up, down, tokens, cot, nzh, nzl):
    rows, d = tokens.shape
    return call(
        functools.partial(prepare_kernel, nzh=nzh, nzl=nzl),
        [struct(*routes.shape, dtype=jnp.int32), struct(*weights.shape, dtype=F32)]
        + [struct(rows, d)] * 2
        + [struct(d // 2, 3 * LANES)] * 2,
        [
            pltpu.VMEM((d, LANES), BF),
            pltpu.VMEM((d, LANES), BF),
            pltpu.VMEM((LANES, d), BF),
            pltpu.VMEM((d, LANES), BF),
            pltpu.SemaphoreType.DMA((7,)),
        ],
        16, 1 << 28, core, routes, weights, gate, up, down, tokens, cot, space=pltpu.HBM,
    )


def pack_kernel(core, routes, weights, x, c, out, sel, xo, wsel, *, experts, cap, nzl):
    half = x.shape[1] // 2
    first, second, rank = ranks(routes[...], experts)
    w = weights[...]
    mine = jnp.where(first, w[0:1], 0.0) + jnp.where(second, w[1:2], 0.0)
    slot = lax.broadcasted_iota(jnp.int32, (cap, rank.shape[1]), 0).astype(F32)
    for e in range(experts):
        hit = rank[e : e + 1] == slot
        sel[pl.ds(e * cap, cap), :] = jnp.where(hit, 1.0, 0.0).astype(BF)
        wsel[pl.ds(e * cap, cap), :] = jnp.where(hit, mine[e : e + 1], 0.0).astype(BF)
    gather_lanes(x, core[0], nzl, xo, 0)
    gather_lanes(c, core[0], nzl, xo, half)
    out[:, pl.ds(0, half)] = dot(sel[...], xo[:, pl.ds(0, half)]).astype(BF)
    out[:, pl.ds(half, half)] = dot(wsel[...], xo[:, pl.ds(half, half)]).astype(BF)


def pack(core, routes, weights, x, c, experts, cap, nzl):
    rows, d = x.shape
    slots = experts * cap
    return call(
        functools.partial(pack_kernel, experts=experts, cap=cap, nzl=nzl),
        [struct(slots, d), struct(slots, rows)],
        [pltpu.VMEM((rows, d), BF), pltpu.VMEM((slots, rows), BF)],
        12, 2 * slots * rows * d, core, routes, weights, x, c,
    )


def forward_kernel(core, own, w_own, w_got, out):
    half = own.shape[1] // 2
    for k, w in enumerate((w_own, w_got)):
        col = 3 * LANES * k
        out[:, pl.ds(col, 2 * LANES)] = dot(own[:, pl.ds(0, half)], w[:, pl.ds(0, 2 * LANES)]).astype(BF)
    down = jnp.concatenate([w[:, pl.ds(2 * LANES, LANES)] for w in (w_own, w_got)], axis=1)
    back = dot(own[:, pl.ds(half, half)], down).astype(BF)
    out[:, pl.ds(2 * LANES, LANES)] = back[:, :LANES]
    out[:, pl.ds(5 * LANES, LANES)] = back[:, LANES:]


def forward(core, own, w_own, w_got):
    slots, d = own.shape
    return call(
        forward_kernel, [struct(slots, 6 * LANES)], [], 20, 6 * slots * d * LANES,
        core, own, w_own, w_got,
    )[0]


def backward_kernel(core, part, got, w_own, w_got, hid, dd, out, *, cap, nzl):
    slots = part.shape[0]
    half = w_own.shape[0]
    per = half // nzl // LANES
    lane = 3 * LANES
    group = slots // 2 if slots % (2 * cap) == 0 else slots
    for i in range(slots // group):
        at = pl.ds(i * group, group)
        route = None
        for k in range(2):

            def total(j):
                cols = [pl.ds(lane * side + LANES * j, LANES) for side in (k, 1 - k)]
                return part[at, cols[0]].astype(F32) + got[at, cols[1]].astype(F32)

            a, b, back = total(0), total(1), total(2)
            s = jax.nn.sigmoid(a)
            act = a * s
            hidden = (act * b).astype(BF)
            hid[at, pl.ds(k * LANES, LANES)] = hidden
            da = (back * b * s * (1.0 + a * (1.0 - s))).astype(BF)
            both = jnp.concatenate([da, (back * act).astype(BF)], axis=1)
            dd[at, pl.ds(2 * k * LANES, 2 * LANES)] = both
            term = dot(both, (w_own, w_got)[k][:, pl.ds(0, 2 * LANES)], 1, 1)
            rows = term if k == 0 else rows + term
            one = jnp.sum((hidden.astype(F32) * back).T, axis=0, keepdims=True)
            route = one if route is None else route + one
        rows = rows.astype(BF)
        for j in range(group // cap):
            b = i * (group // cap) + j
            ends = stacked(split(padded(route[:, j * cap : (j + 1) * cap], LANES)), 8).astype(BF)
            for zl in range(nzl):
                for q in range(per):
                    k = zl * per + q
                    out[zl * (slots // cap) + b, pl.ds(q * cap, cap), :] = rows[
                        j * cap : (j + 1) * cap, k * LANES : (k + 1) * LANES
                    ]
                out[zl * (slots // cap) + b, pl.ds(per * cap, 8), :] = ends


def backward(core, part, got, w_own, w_got, nzl, cap):
    slots, half = part.shape[0], w_own.shape[0]
    tall = half // nzl // LANES * cap + 8
    return call(
        functools.partial(backward_kernel, cap=cap, nzl=nzl),
        [
            struct(slots, 2 * LANES),
            struct(slots, 4 * LANES),
            struct(slots // cap * nzl, tall, LANES),
        ],
        [], 24, 8 * slots * half * LANES, core, part, got, w_own, w_got,
    )


def grads_kernel(core, own, hid, dd, keep, send):
    half = own.shape[1] // 2
    both = dot(own[:, pl.ds(0, half)], dd[...], 0, 0)
    keep[:, pl.ds(0, 2 * LANES)] = both[:, : 2 * LANES].astype(BF)
    send[:, pl.ds(0, 2 * LANES)] = both[:, 2 * LANES :].astype(BF)
    down = dot(own[:, pl.ds(half, half)], hid[...], 0, 0)
    keep[:, pl.ds(2 * LANES, LANES)] = down[:, :LANES].astype(BF)
    send[:, pl.ds(2 * LANES, LANES)] = down[:, LANES:].astype(BF)


def grads(core, own, hid, dd):
    slots, d = own.shape
    return call(
        grads_kernel, [struct(d // 2, 3 * LANES)] * 2, [], 24,
        6 * slots * d * LANES, core, own, hid, dd,
    )


def place_kernel(core, keep, got, gg, gu, gd, turned, *, nzh, nzl):
    for k, out in enumerate((gg, gu, turned)):
        for src, who in ((keep, core[0]), (got, 1 - core[0])):
            for at, to in blocks(who, nzh, nzl):
                out[to, :] = src[at, pl.ds(k * LANES, LANES)]
    gd[...] = turned[...].T


def place(core, keep, got, nzh, nzl):
    d = 2 * keep.shape[0]
    return call(
        functools.partial(place_kernel, nzh=nzh, nzl=nzl),
        [struct(d, LANES), struct(d, LANES), struct(LANES, d)],
        [pltpu.VMEM((d, LANES), BF)],
        12, 1 << 28, core, keep, got,
    )


def combine_kernel(routes, weights, sel, got, out, part, *, experts, cap, nzl):
    rows = routes.shape[1]
    per = (got.shape[1] - 8) // cap
    s = sel[...]
    total = None
    for zl in range(nzl):
        for e in range(experts):
            for q in range(per):
                part[zl, pl.ds(e * cap, cap), pl.ds(q * LANES, LANES)] = got[
                    zl * experts + e, pl.ds(q * cap, cap), :
                ]
        one = dot(s, part[zl], 0, 0)
        total = one if total is None else total + one
    total = total.astype(BF)
    mid = rows // 2
    for k in range(out.shape[0]):
        out[k, pl.ds(0, mid), :] = jnp.concatenate(
            [total[:mid, k * OWN : (k + 1) * OWN], total[mid:, k * OWN : (k + 1) * OWN]], axis=1
        )
    lines = []
    for e in range(experts):
        line = jnp.zeros((1, LANES), F32)
        for zl in range(nzl):
            tail = got[zl * experts + e, pl.ds(per * cap, 8), :].astype(F32)
            line = line + tail[0:1] + tail[1:2]
        lines.append(line)
    r_hi, r_lo = split(stacked(lines, max(experts, 8)))
    first, second, rank = ranks(routes[...], experts)
    slot = lax.broadcasted_iota(jnp.int32, (LANES, rows), 0).astype(F32)
    ends = []
    wide = -(-rows // LANES) * LANES
    for ch, hit in enumerate((first, second)):
        place = jnp.sum(jnp.where(hit, rank, 0.0), axis=0, keepdims=True)
        pick = jnp.where(slot == place, 1.0, 0.0).astype(BF)
        value = (dot(r_hi, pick) + dot(r_lo, pick))[:experts]
        value = jnp.sum(jnp.where(hit, value, 0.0), axis=0, keepdims=True)
        w = weights[...][ch : ch + 1].astype(BF).astype(F32)
        for piece in split(padded(value / w, wide) if wide > rows else value / w):
            for k in range(wide // LANES):
                ends.append(piece[:, k * LANES : (k + 1) * LANES])
    ends = stacked(ends, 8).astype(BF)
    for k in range(out.shape[0]):
        out[k, pl.ds(mid, 8), :] = ends


def combine(routes, weights, sel, got, experts, cap, nzh, nzl):
    rows = routes.shape[1]
    per = (got.shape[1] - 8) // cap
    return pl.pallas_call(
        functools.partial(combine_kernel, experts=experts, cap=cap, nzl=nzl),
        out_shape=jax.ShapeDtypeStruct((nzh, rows // 2 + 8, LANES), BF),
        in_specs=vmem(4),
        out_specs=vmem(1)[0],
        scratch_shapes=[pltpu.VMEM((nzl, experts * cap, per * LANES), BF)],
        compiler_params=pltpu.CompilerParams(vmem_limit_bytes=16 << 20),
        name="combine",
    )(routes, weights, sel, got)


def finish_kernel(got, grad, route):
    rows = grad.shape[1]
    total = got[0].astype(F32)
    for k in range(1, got.shape[0]):
        total = total + got[k].astype(F32)
    mid = rows // 2
    turned = total[:mid].T
    grad[...] = jnp.concatenate([turned[:OWN], turned[OWN:]], axis=1).astype(BF)
    ends = total[mid:]
    n = -(-rows // LANES)
    for ch in range(2):
        pieces = [
            ends[2 * n * ch + k : 2 * n * ch + k + 1] + ends[2 * n * ch + n + k : 2 * n * ch + n + k + 1]
            for k in range(n)
        ]
        line = jnp.concatenate(pieces, axis=1) if n > 1 else pieces[0]
        route[pl.ds(ch, 1), :] = line[:, :rows]


def finish(got, rows):
    return pl.pallas_call(
        finish_kernel,
        out_shape=[
            jax.ShapeDtypeStruct((OWN, rows), BF),
            jax.ShapeDtypeStruct((2, rows), F32),
        ],
        in_specs=vmem(1),
        out_specs=vmem(2),
        compiler_params=pltpu.CompilerParams(vmem_limit_bytes=8 << 20),
        name="finish",
    )(got)


def shards(tokens, cotangent, routes, route_weight, gate_weight, up_weight, down_weight):
    rows, d = tokens.shape
    experts = lax.axis_size("ep")
    nzh, nzl = lax.axis_size("zh"), lax.axis_size("zl")
    cap = 2 * rows * routes.shape[1] // experts
    slots = experts * cap
    core = lax.axis_index("core").astype(jnp.int32).reshape(1)
    routes_t, weight_t = routes.T, route_weight.T
    gate, up, down = gate_weight[0], up_weight[0], down_weight[0]
    swap = [(0, 1), (1, 0)]

    routes_v, weight_v, x_v, c_v, w_own, w_oth = prepare(
        core, routes_t, weight_t, gate, up, down, tokens, cotangent, nzh, nzl
    )
    w_got = lax.ppermute(w_oth, "core", swap)
    packed, sel = pack(core, routes_v, weight_v, x_v, c_v, experts, cap, nzl)
    packed, w_own, w_got = lax.optimization_barrier((packed, w_own, w_got))
    own = lax.all_to_all(packed.reshape(experts, cap, d), "ep", 0, 0, tiled=True).reshape(slots, d)
    part = forward(core, own, w_own, w_got)
    got = lax.ppermute(part, "core", swap)
    hid, dd, message = backward(core, part, got, w_own, w_got, nzl, cap)
    keep, send = grads(core, own, hid, dd)
    moved = lax.ppermute(send, "core", swap)
    gg, gu, gd = place(core, keep, moved, nzh, nzl)
    back = lax.all_to_all(message, ("zl", "ep"), 0, 0, tiled=True)
    partial = combine(routes_v, weight_v, sel, back, experts, cap, nzh, nzl)
    last = lax.all_to_all(partial, "zh", 0, 0, tiled=True)
    grad_t, route_t = finish(last, rows)
    return grad_t.T, route_t.T, gg[None], gu[None], gd[None]


def solution(mesh):
    devices = mesh.devices
    ep = devices.shape[0]
    finer = Mesh(devices.reshape(ep, -1, 2, 2), ("ep", "zh", "zl", "core"))
    in_specs = (
        P("ep", None),
        P("ep", None),
        P("ep", None),
        P("ep", None),
        P("ep", None, TP),
        P("ep", None, TP),
        P("ep", TP, None),
    )
    out_specs = (
        P("ep", TP),
        P("ep", None),
        P("ep", None, TP),
        P("ep", None, TP),
        P("ep", TP, None),
    )
    return jax.shard_map(
        shards, mesh=finer, in_specs=in_specs, out_specs=out_specs, check_vma=False
    )
```
